512 devices in a mesh: sp: 32 (over z, x), tp: 16 (over y, core).
Axes of the slice: x: 4, y: 8, z: 8, core: 2. Of those that a mesh axis runs over, the one named last changes fastest.
Arguments:
- pool_input: bfloat16 [8192, 1024], P('sp', 'tp'), may hold values from -6 to 6
- pool_weight: bfloat16 [16, 64, 64], P('tp'), may hold values from -0.75 to 0.75
- pool_gain: bfloat16 [1024], P('tp'), may hold values from 0.099609375 to 1.8984375
- out_weight: bfloat16 [1024, 2048], P(None, 'tp'), may hold values from -0.1875 to 0.1875
- resid: bfloat16 [8192, 2048], P('sp', 'tp'), may hold values from -90 to 90
- norm_gain: bfloat16 [2048], P('tp'), may hold values from 0.099609375 to 1.8984375
- routes: int32 [8192, 2], P('sp'), may hold values from 0 to 31, all different within a row; in each aligned block of 256 rows (0 to 255, 256 to 511, ...) at most 32 rows name the same one
- route_weight: float32 [8192, 2], P('sp'), may hold values from 0.2 to 1
- expert_gate: bfloat16 [32, 2048, 4096], P('sp', None, 'tp'), may hold values from -0.375 to 0.375
- expert_up: bfloat16 [32, 2048, 4096], P('sp', None, 'tp'), may hold values from -0.375 to 0.375
- expert_down: bfloat16 [32, 4096, 2048], P('sp', 'tp'), may hold values from -0.0234375 to 0.0234375
Outputs:
- layer_out: bfloat16 [8192, 2048], P('sp', 'tp')
The draws below stay inside these ranges and needn't reach their ends.
Inputs may be any that keep to these rules, and one draw needn't show every extreme that they name: `routes`: the 2 experts of a position differ. In each aligned block of 256 positions no expert is named by more than 32 assignments; some block reaches that bound.
All inputs are finite; a program needn't handle non-finite values.
Results may differ from the reference program's by a relative error of at most 0.0085.
Values may be sent and summed in bfloat16 or wider, within the bound.
No kernel may reach another device: no remote copies, remote signals or barrier semaphores. Data moves between devices by JAX's collectives and lax.ppermute only.
A program may use at most 64 MiB of HBM per device.

```python
import math
from functools import partial
import jax
import jax.numpy as jnp
import numpy as np
from jax import lax

D = 2048
FF = 4096
GSIZE = 64
REACH = 16
TOPK = 2
TOK_SP = 256
GROUPS = 16
PW = 1024
EXPERTS = 32
CAP = 32
TOKENS = 8192
N_SP = 32
N_TP = 16


def draw_resid(key, part):
    key_jitter, key_rows = jax.random.split(key, 2)
    column = 0.3 * 10.0 ** (jnp.arange(D, dtype=jnp.float32) / D)
    jitter = jnp.clip(jax.random.normal(key_jitter, (TOKENS, D), jnp.float32), -6.0, 6.0)
    spread = jax.random.uniform(key_rows, (TOKENS, 1), jnp.float32, 0.0, 0.5)
    return (jitter * column * 10.0 ** spread).astype(jnp.bfloat16)


def spiked(values, stream_key, source, target, parts, factor):
    def block_of(dim):
        return (jnp.arange(values.shape[dim]) // (values.shape[dim] // parts)).reshape((-1,) + (1,) * (values.ndim - 1 - dim))

    near = jax.random.permutation(stream_key, parts)[block_of(target)]
    other_side = (block_of(target) + parts // 2) % parts
    return jnp.where((block_of(source) == near) | (block_of(source) == other_side), factor * values, values)


def block_levels(key, shape, pieces, smallest, largest):
    gain, own = 1.0, jax.random.fold_in(key, 6)
    for dim, shards_of in pieces:
        draws = jnp.exp(jax.random.uniform(jax.random.fold_in(own, dim), (shards_of,), jnp.float32, smallest / len(pieces), largest / len(pieces)))
        gain = gain * jnp.repeat(draws, shape[dim] // shards_of).reshape([-1 if axis == dim else 1 for axis in range(len(shape))])
    return gain


def routed_block(own_key, own, number, rows, amount, top, bound, slope):
    sequence = jax.random.permutation(own_key, amount)
    crowded, usual = shares(amount, rows * top, bound, slope, True), shares(amount, rows * top, bound, slope, False)
    places = jnp.arange(amount)

    def named(lengths, turn):
        used = int((lengths > 0).sum())
        fixed = max(1, used // 4)
        passed = fixed + (places - fixed + turn * (used - fixed)) % max(1, amount - fixed)
        return jnp.zeros((amount,), jnp.int32).at[sequence[jnp.where(places < fixed, places, passed)]].set(jnp.asarray(lengths, jnp.int32))

    lengths = jnp.where(number % 4 == 0, named(crowded, number // 4), named(usual, number - number // 4 - 1))
    mixed = jax.random.permutation(jax.random.fold_in(own, 3), amount)
    donor, receiver = mixed[0:amount // 2 * 2:2], mixed[1:amount // 2 * 2:2]
    margin = jnp.minimum(lengths[donor] - 1, bound - lengths[receiver]) // 2
    margin = jnp.where((donor == sequence[0]) | (receiver == sequence[0]) | (lengths[receiver] == 0), 0, jnp.maximum(margin, 0))
    passed = jax.random.randint(jax.random.fold_in(own, 4), (amount // 2,), 0, 1 << 20) % (margin + 1)
    lengths = lengths.at[donor].add(-passed).at[receiver].add(passed)
    items = jnp.searchsorted(jnp.cumsum(lengths), jnp.arange(rows * top), side="right").astype(jnp.int32)
    listing = items.reshape(top, rows).T
    listing = listing[jax.random.permutation(jax.random.fold_in(own, 1), rows)]
    turn = jax.random.randint(jax.random.fold_in(own, 2), (rows, 1), 0, top)
    return jnp.take_along_axis(listing, (jnp.arange(top)[None, :] + turn) % top, axis=1)


def shares(amount, total, bound, skew, full):
    weights = [(1 << 20) // math.isqrt(rank ** skew) + 1 for rank in range(1, amount + 1)]
    largest = bound if full else min(bound, max(-(-total // amount), total * weights[0] // sum(weights)))
    least = 1 if total - largest >= amount - 1 else 0
    holding, surplus = [largest] + [least] * (amount - 1), total - largest - least * (amount - 1)
    while surplus > 0:
        movable = [i for i in range(1, amount) if holding[i] < largest] or [i for i in range(1, amount) if holding[i] < bound]
        mass, remaining = sum([weights[i] for i in movable]), surplus
        for i in movable:
            more = min(bound - holding[i], max(1, remaining * weights[i] // mass), surplus)
            holding[i] = holding[i] + more
            surplus = surplus - more
    return np.array(holding)


def bell_draw(key, shape, scale, limit, pieces=(), kind=jnp.bfloat16):
    factor_of = block_levels(key, shape, pieces, -0.22, 0.18) if pieces else 1.0
    entries = jax.random.normal(key, shape, jnp.float32) * scale * factor_of
    return jnp.minimum(jnp.maximum(entries, -limit), limit).astype(kind)


def heavy_noise(own_key, extent, scale, most, cuts, heavy, held_as=jnp.bfloat16):
    entries = scale * jax.random.normal(own_key, extent, jnp.float32)
    if cuts:
        entries = entries * block_levels(own_key, extent, cuts, -0.22, 0.18)
    return jnp.clip(spiked(entries, jax.random.fold_in(own_key, 3), *heavy), -most, most).astype(held_as)


def setup_inputs(seed: int = 0) -> dict:
    arg_keys = jax.random.split(jax.random.key(seed), 12)
    pool_input = bell_draw(arg_keys[0], (TOKENS, PW), 1.0, 6.0, ((0, 32), (1, 16)))
    pool_weight = bell_draw(arg_keys[1], (GROUPS, GSIZE, GSIZE), GSIZE ** -0.5, 0.75, ((0, 16),))
    pool_gain = jnp.clip(1.0 + 0.18 * jax.random.normal(arg_keys[2], (PW,), jnp.float32), 0.099609375, 1.8984375).astype(jnp.bfloat16)
    out_weight = bell_draw(arg_keys[3], (PW, D), PW ** -0.5, 0.1875, ((1, 16),))
    resid = draw_resid(jax.random.fold_in(arg_keys[11], 71), 0)
    norm_gain = jnp.clip(1.0 + 0.18 * jax.random.normal(arg_keys[5], (D,), jnp.float32), 0.099609375, 1.8984375).astype(jnp.bfloat16)
    routes_keys = jax.random.split(jax.random.fold_in(arg_keys[6], 1), TOKENS // TOK_SP)
    routes_turns = jax.random.permutation(jax.random.fold_in(arg_keys[6], 3), TOKENS // TOK_SP)
    routes = jax.vmap(lambda own, number: routed_block(jax.random.fold_in(arg_keys[6], 2), own, number, TOK_SP, EXPERTS, TOPK, CAP, 1))(routes_keys, routes_turns).reshape((TOKENS, TOPK))
    route_weight = jnp.clip(0.2 + 0.8 * jax.random.uniform(arg_keys[7], (TOKENS, TOPK), jnp.float32) ** block_levels(arg_keys[7], (TOKENS, TOPK), ((0, 32),), -0.2, 0.2), 0.2, 1.0)
    expert_gate = bell_draw(arg_keys[8], (EXPERTS, D, FF), (D // 9) ** -0.5, 0.375, ((0, 32), (2, 16)))
    expert_up = bell_draw(arg_keys[9], (EXPERTS, D, FF), (D // 9) ** -0.5, 0.375, ((0, 32), (2, 16)))
    expert_down = heavy_noise(arg_keys[10], (EXPERTS, FF, D), (FF * 32) ** -0.5, 0.0234375, ((0, 32), (1, 16)), (1, 2, 16, 2.0))
    return {"pool_input": pool_input, "pool_weight": pool_weight, "pool_gain": pool_gain, "out_weight": out_weight, "resid": resid, "norm_gain": norm_gain, "routes": routes, "route_weight": route_weight, "expert_gate": expert_gate, "expert_up": expert_up, "expert_down": expert_down}


GATE_LIMIT = 7.0
GATE_ALPHA = 1.702
NORM_EPS = 1e-05

def clamped_unit(gate_pre, up_pre):
    gate_cut = jnp.minimum(gate_pre, GATE_LIMIT)
    up_cut = jnp.clip(up_pre, -GATE_LIMIT, GATE_LIMIT)
    return (up_cut + 1.0) * gate_cut * jax.nn.sigmoid(GATE_ALPHA * gate_cut)

def window_pool(extended, width_of, position, tok_count):
    summed = jnp.zeros((tok_count, extended.shape[1]), jnp.float32)
    for offset in range(REACH):
        first_row = REACH - 1 - offset
        shifted = extended[first_row:first_row + tok_count]
        summed = summed + jnp.where(offset < width_of[None, :], shifted, 0.0)
    counted = jnp.minimum(position[:, None] + 1, width_of[None, :]).astype(jnp.float32)
    current = extended[REACH - 1:]
    return (summed / counted - current).astype(jnp.bfloat16)

def slot_of(route_block, expert_count, capacity):
    flattened = route_block.reshape(-1).astype(jnp.int32)
    onehot = (flattened[:, None] == jnp.arange(expert_count, dtype=jnp.int32)[None, :]).astype(jnp.int32)
    earlier = (jnp.cumsum(onehot, axis=0) - onehot).astype(jnp.int32)
    ranked = lax.optimization_barrier(jnp.sum(earlier * onehot, axis=1)).astype(jnp.int32)
    return (flattened * capacity + ranked).astype(jnp.int32)

def fill_table(slot_row, id_row, weight_row):
    id_table = jnp.full((EXPERTS * CAP,), TOKENS, jnp.int32).at[slot_row].set(id_row)
    weight_table = jnp.zeros((EXPERTS * CAP,), jnp.float32).at[slot_row].set(weight_row)
    return (id_table, weight_table)

def reference(pool_input, pool_weight, pool_gain, out_weight, resid, norm_gain, routes, route_weight, expert_gate, expert_up, expert_down):
    channels = pool_input.shape[1]
    width_of = 2 ** (1 + jnp.arange(channels, dtype=jnp.int32) // GSIZE % 4)
    position = jnp.arange(TOKENS, dtype=jnp.int32)
    extended = jnp.concatenate([jnp.zeros((REACH - 1, channels), jnp.float32), pool_input.astype(jnp.float32)], axis=0)
    pooled = window_pool(extended, width_of, position, TOKENS)
    grouped = jnp.einsum('tgc,gcd->tgd', pooled.reshape(TOKENS, GROUPS, GSIZE).astype(jnp.float32), pool_weight.astype(jnp.float32))
    mixed_out = (grouped * pool_gain.astype(jnp.float32).reshape(GROUPS, GSIZE)).astype(jnp.bfloat16).reshape(TOKENS, PW)
    projected = jnp.dot(mixed_out, out_weight, preferred_element_type=jnp.float32)
    stored = lax.optimization_barrier((resid.astype(jnp.float32) + projected).astype(jnp.bfloat16))
    stream = stored.astype(jnp.float32)
    scale_row = lax.rsqrt(lax.optimization_barrier(jnp.mean(stream * stream, axis=1, keepdims=True)) + NORM_EPS)
    normed = (stream * scale_row * norm_gain.astype(jnp.float32)).astype(jnp.bfloat16)
    slots = jax.vmap(partial(slot_of, expert_count=EXPERTS, capacity=CAP))(routes.reshape(N_SP, TOK_SP, TOPK))
    token_ids = jnp.repeat(jnp.arange(TOKENS, dtype=jnp.int32), TOPK).reshape(N_SP, TOK_SP * TOPK)
    weights = route_weight.astype(jnp.float32).reshape(N_SP, TOK_SP * TOPK)
    id_tables, weight_tables = jax.vmap(fill_table)(slots, token_ids, weights)
    id_tables = id_tables.reshape(N_SP, EXPERTS, CAP).transpose(1, 0, 2).reshape(EXPERTS, N_SP * CAP)
    weight_tables = weight_tables.reshape(N_SP, EXPERTS, CAP).transpose(1, 0, 2).reshape(EXPERTS, N_SP * CAP)
    hidden_part = FF // N_TP

    def expert_step(running, inputs):
        id_row, weight_row, gate_w, up_w, down_w = inputs
        chosen = jnp.take(normed, id_row, axis=0, mode='fill', fill_value=0)
        gate_pre = jnp.dot(chosen, gate_w, preferred_element_type=jnp.float32)
        up_pre = jnp.dot(chosen, up_w, preferred_element_type=jnp.float32)
        hidden = clamped_unit(gate_pre, up_pre).astype(jnp.bfloat16)
        summed = jnp.zeros((id_row.shape[0], D), jnp.float32)
        for block_idx in range(N_TP):
            lower = block_idx * hidden_part
            partial_out = jnp.dot(hidden[:, lower:lower + hidden_part], down_w[lower:lower + hidden_part], preferred_element_type=jnp.float32)
            rounded = lax.optimization_barrier(partial_out.astype(jnp.bfloat16))
            summed = summed + rounded.astype(jnp.float32)
        output_rows = lax.optimization_barrier(summed.astype(jnp.bfloat16)).astype(jnp.float32)
        running = running.at[id_row].add(output_rows * weight_row[:, None], mode='drop')
        return (running, None)
    running, ignored = lax.scan(expert_step, jnp.zeros((TOKENS, D), jnp.float32), (id_tables, weight_tables, expert_gate, expert_up, expert_down))
    return (stream + running).astype(jnp.bfloat16)
```

```python
import functools

import jax
import jax.numpy as jnp
from jax import lax
from jax.experimental import pallas as pl
from jax.experimental.pallas import tpu as pltpu
from jax.sharding import PartitionSpec as P


GSIZE = 64
REACH = 16
TOPK = 2
CORES = 2

GATE_LIMIT = 7.0
GATE_ALPHA = 1.702
NORM_EPS = 1e-05

F32 = jnp.float32
BF16 = jnp.bfloat16
MIB = 1024 * 1024


def iota(shape, dim):
    return lax.broadcasted_iota(jnp.int32, shape, dim)


def mm(a, b, ca=1, cb=0):
    return lax.dot_general(a, b, (((ca,), (cb,)), ((), ())), preferred_element_type=F32)


def call(kernel, out_shape, args, flops, mib, aliases=None):
    return pl.pallas_call(
        kernel,
        out_shape=out_shape,
        in_specs=[pl.BlockSpec(memory_space=pltpu.VMEM)] * len(args),
        out_specs=jax.tree.map(lambda _: pl.BlockSpec(memory_space=pltpu.VMEM), out_shape),
        compiler_params=pltpu.CompilerParams(vmem_limit_bytes=mib * MIB),
        cost_estimate=pl.CostEstimate(flops=flops, bytes_accessed=flops // 512, transcendentals=0),
        input_output_aliases=aliases or {},
    )(*args)


def pool_kernel(before_ref, x_ref, w_ref, gain_ref, norm_ref, out_ref):
    rows, width = x_ref.shape
    window = lax.shift_left(jnp.int32(2), lax.rem(lax.axis_index("tp"), 4))
    place = iota((rows, rows), 0) - iota((rows, rows), 1)
    inside = jnp.where((place >= 0) & (place < window), 1.0, 0.0).astype(BF16)
    gap = iota((rows, REACH), 0) + REACH - iota((rows, REACH), 1)
    behind = jnp.where(gap < window, 1.0, 0.0).astype(BF16)
    x = x_ref[...]
    total = mm(inside, x) + mm(behind, before_ref[...])
    spot = lax.axis_index("sp") * rows + iota((rows, 1), 0)
    count = jnp.minimum(spot + 1, window).astype(F32)
    pooled = (total / count - x.astype(F32)).astype(BF16)
    mixed = (mm(pooled, w_ref[...]) * gain_ref[...].astype(F32)).astype(BF16)
    eye = jnp.where(iota((width, width), 0) == iota((width, width), 1), 1.0, 0.0).astype(BF16)
    out_ref[:width, :] = mm(eye, mixed, 1, 1).astype(BF16)
    features = norm_ref.shape[1]
    tail = out_ref.shape[0] - width
    out_ref[width:, :features] = jnp.broadcast_to(norm_ref[...].astype(F32), (tail, features)).astype(BF16)
    out_ref[width:, features:] = jnp.zeros((tail, out_ref.shape[1] - features), BF16)


def stream_kernel(mixed_ref, w_ref, resid_ref, out_ref, gain_ref):
    members, _, rows = mixed_ref.shape
    mixed = mixed_ref[:, :GSIZE, :].reshape(members * GSIZE, rows)
    projected = mm(mixed, w_ref[...], 0, 0)
    out_ref[...] = (resid_ref[...].astype(F32) + projected).astype(BF16)
    features = out_ref.shape[1]
    for t in range(members):
        y, c = divmod(t, CORES)
        row = mixed_ref[t, GSIZE : GSIZE + 8, :features].astype(F32)
        gain_ref[y, :, c * features : (c + 1) * features] = row


def row_slots(routes_ref, experts, capacity):
    rows = routes_ref.shape[1]
    named = [iota((experts, rows), 0) == routes_ref[k : k + 1, :] for k in range(TOPK)]
    ones = sum(jnp.where(n, 1.0, 0.0) for n in named)
    upper = jnp.where(iota((rows, rows), 0) < iota((rows, rows), 1), 1.0, 0.0).astype(BF16)
    earlier = mm(ones.astype(BF16), upper)
    slots = []
    for k in range(TOPK):
        rank = jnp.sum(jnp.where(named[k], earlier, 0.0), axis=0, keepdims=True).astype(jnp.int32)
        slots.append(routes_ref[k : k + 1, :] * capacity + rank)
    return slots


def column_slots(routes_ref, experts, capacity):
    rows = routes_ref.shape[0]
    named = [iota((rows, experts), 1) == routes_ref[:, k : k + 1] for k in range(TOPK)]
    ones = sum(jnp.where(n, 1.0, 0.0) for n in named)
    lower = jnp.where(iota((rows, rows), 0) > iota((rows, rows), 1), 1.0, 0.0).astype(BF16)
    earlier = mm(lower, ones.astype(BF16))
    slots = []
    for k in range(TOPK):
        rank = jnp.sum(jnp.where(named[k], earlier, 0.0), axis=1, keepdims=True).astype(jnp.int32)
        slots.append(routes_ref[:, k : k + 1] * capacity + rank)
    return slots


def slot_ids(shape, dim, capacity, core):
    half = capacity // CORES
    place = iota(shape, dim)
    return lax.div(place, half) * capacity + core * half + lax.rem(place, half)


def dispatch_kernel(experts, capacity, own_ref, other_ref, routes_ref, out_ref):
    core = lax.rem(lax.axis_index("tp"), CORES)
    slots = row_slots(routes_ref, experts, capacity)
    shape = (out_ref.shape[0], own_ref.shape[0])
    ids = slot_ids(shape, 0, capacity, core)
    hit = (slots[0] == ids) | (slots[1] == ids)
    chosen = jnp.where(hit, 1.0, 0.0).astype(BF16)
    features = own_ref.shape[1]
    own = mm(chosen, own_ref[...]).astype(BF16)
    other = mm(chosen, other_ref[...]).astype(BF16)
    out_ref[:, :features] = jnp.where(core == 0, own, other)
    out_ref[:, features:] = jnp.where(core == 0, other, own)


def add_chunk(x, chip, gain_ref, weights, acc_ref, square_ref, first=False):
    width = x.shape[1]
    value = x.astype(F32)
    square = value * value
    lanes = square_ref.shape[1]
    square = sum(square[:, i : i + lanes] for i in range(0, width, lanes))
    scaled = (value * gain_ref[chip, 0:1, :]).astype(BF16)
    rows = pl.ds(pl.multiple_of(chip * width, width), width)
    columns = weights[0].shape[1]
    for i, w in enumerate(weights):
        part = mm(scaled, w[rows, :])
        span = slice(i * columns, (i + 1) * columns)
        acc_ref[:, span] = part if first else acc_ref[:, span] + part
    square_ref[...] = square if first else square_ref[...] + square


def chip_at(chips, step):
    here = lax.div(lax.axis_index("tp"), CORES)
    return lax.rem(here + step + chips, chips)


def first_kernel(chips, x_ref, gain_ref, a_ref, b_ref, c_ref, d_ref, acc_ref, square_ref):
    add_chunk(x_ref[...], chip_at(chips, 0), gain_ref, (a_ref, b_ref, c_ref, d_ref), acc_ref, square_ref, True)


def both_kernel(chips, step, p_ref, m_ref, gain_ref, a_ref, b_ref, c_ref, d_ref, acc_in, square_in, acc_ref, square_ref):
    weights = (a_ref, b_ref, c_ref, d_ref)
    add_chunk(p_ref[...], chip_at(chips, -step), gain_ref, weights, acc_ref, square_ref)
    add_chunk(m_ref[...], chip_at(chips, step), gain_ref, weights, acc_ref, square_ref)


def partial(hidden_ref, down_refs, chip, width):
    columns = pl.ds(pl.multiple_of(chip * width, width), width)
    units = down_refs[0].shape[0]
    return sum(mm(hidden_ref[:, i * units : (i + 1) * units], d[:, columns]) for i, d in enumerate(down_refs))


def last_kernel(
    chips, total, p_ref, m_ref, gain_ref, a_ref, b_ref, c_ref, d_ref, acc_in, square_in, e_ref, f_ref,
    hidden_ref, up_ref, low_ref, acc_ref, square_ref,
):
    x = jnp.concatenate([p_ref[...], m_ref[...]], axis=0)
    weights = (a_ref, b_ref, c_ref, d_ref)
    far = chip_at(chips, chips // 2)
    acc_ref[...] = acc_in[...]
    square_ref[...] = square_in[...]
    add_chunk(x, far, gain_ref, weights, acc_ref, square_ref)
    mean = jnp.sum(square_ref[...], axis=1, keepdims=True) / total
    scale = lax.rsqrt(mean + NORM_EPS)
    units = hidden_ref.shape[1]
    gate = jnp.minimum(acc_ref[:, :units] * scale, GATE_LIMIT)
    up = jnp.clip(acc_ref[:, units:] * scale, -GATE_LIMIT, GATE_LIMIT)
    hidden_ref[...] = ((up + 1.0) * gate * jax.nn.sigmoid(GATE_ALPHA * gate)).astype(BF16)
    out = partial(hidden_ref, (e_ref, f_ref), far, x.shape[1]).astype(BF16)
    half = up_ref.shape[0]
    up_ref[...] = out[:half]
    low_ref[...] = out[half:]


def down_kernel(chips, step, hidden_ref, e_ref, f_ref, p_ref, m_ref, sp_ref, sm_ref):
    rows, width = sp_ref.shape
    downs = (e_ref, f_ref)
    ahead = partial(hidden_ref, downs, chip_at(chips, step), width)
    back = partial(hidden_ref, downs, chip_at(chips, -step), width)
    held = p_ref.shape[0]
    if held == rows:
        sp_ref[...] = (ahead + p_ref[...].astype(F32)).astype(BF16)
        sm_ref[...] = (back + m_ref[...].astype(F32)).astype(BF16)
    else:
        sp_ref[:held, :] = (ahead[:held] + p_ref[...].astype(F32)).astype(BF16)
        sp_ref[held:, :] = ahead[held:].astype(BF16)
        sm_ref[held:, :] = (back[held:] + m_ref[...].astype(F32)).astype(BF16)
        sm_ref[:held, :] = back[:held].astype(BF16)


def own_kernel(chips, hidden_ref, e_ref, f_ref, p_ref, m_ref, out_ref):
    mine = partial(hidden_ref, (e_ref, f_ref), chip_at(chips, 0), out_ref.shape[1])
    out_ref[...] = (mine + p_ref[...].astype(F32) + m_ref[...].astype(F32)).astype(BF16)


def pick_kernel(experts, capacity, back_ref, routes_ref, weight_ref, mine_ref, other_ref):
    core = lax.rem(lax.axis_index("tp"), CORES)
    slots = column_slots(routes_ref, experts, capacity)
    shape = (routes_ref.shape[0], back_ref.shape[0])
    ids = slot_ids(shape, 1, capacity, core)
    rows = back_ref[...]
    total = 0.0
    for k in range(TOPK):
        chosen = jnp.where(slots[k] == ids, 1.0, 0.0).astype(BF16)
        total = total + mm(chosen, rows) * weight_ref[:, k : k + 1]
    features = mine_ref.shape[1]
    left, right = total[:, :features], total[:, features:]
    mine_ref[...] = jnp.where(core == 0, left, right)
    other_ref[...] = jnp.where(core == 0, right, left)


def join_kernel(stream_ref, mine_ref, other_ref, out_ref):
    out_ref[...] = (stream_ref[...].astype(F32) + mine_ref[...] + other_ref[...]).astype(BF16)


def on_device(
    pool_input,
    pool_weight,
    pool_gain,
    out_weight,
    resid,
    norm_gain,
    routes,
    route_weight,
    expert_gate,
    expert_up,
    expert_down,
):
    tok_rows, channels = pool_input.shape
    features = out_weight.shape[1]
    blocks, members = lax.axis_size("sp"), lax.axis_size("tp")
    chips = members // CORES
    experts = blocks * expert_gate.shape[0]
    capacity = 2 * tok_rows * TOPK // experts
    half = capacity // CORES
    width = features * CORES
    total = features * members
    held = blocks * half

    def along(value, step):
        pairs = [
            (y * CORES + c, (y + step) % chips * CORES + c) for y in range(chips) for c in range(CORES)
        ]
        return lax.ppermute(value, "tp", pairs)

    def across(value):
        return lax.ppermute(value, "tp", [(t, t ^ 1) for t in range(members)])

    before = lax.ppermute(
        pool_input[tok_rows - REACH :], "sp", [(s, s + 1) for s in range(blocks - 1)]
    )
    pooled = call(
        pool_kernel,
        jax.ShapeDtypeStruct((GSIZE + 16, tok_rows), BF16),
        (before, pool_input, pool_weight[0], pool_gain.reshape(1, channels), norm_gain.reshape(1, features)),
        tok_rows * tok_rows * channels * 2,
        8,
    )
    mixed = lax.all_gather(pooled, "tp", axis=0, tiled=False)
    stored, gains = call(
        stream_kernel,
        (
            jax.ShapeDtypeStruct((tok_rows, features), BF16),
            jax.ShapeDtypeStruct((chips, 8, width), F32),
        ),
        (mixed, out_weight, resid),
        2 * tok_rows * features * members * GSIZE,
        8,
    )
    sent = call(
        functools.partial(dispatch_kernel, experts, capacity),
        jax.ShapeDtypeStruct((experts * half, width), BF16),
        (stored, across(stored), routes.T),
        2 * experts * half * width * tok_rows,
        12,
    )
    own = lax.all_to_all(
        sent.reshape(experts, half, width), "sp", split_axis=0, concat_axis=0, tiled=True
    ).reshape(held, width)

    gate, up, down = expert_gate[0], expert_up[0], expert_down[0]
    units = gate.shape[1]
    weights = (gate, across(gate), up, across(up))
    downs = (down, across(down))
    acc_shape = (
        jax.ShapeDtypeStruct((held, 4 * units), F32),
        jax.ShapeDtypeStruct((held, 128), F32),
    )
    chunk_flops = 2 * held * width * 4 * units
    acc, square = call(
        functools.partial(first_kernel, chips), acc_shape, (own, gains, *weights), chunk_flops, 16
    )
    ahead, back = own, own
    middle = held // 2
    for step in range(1, chips // 2):
        ahead, back = along(ahead, 1), along(back, -1)
        acc, square = call(
            functools.partial(both_kernel, chips, step),
            acc_shape,
            (ahead, back, gains, *weights, acc, square),
            2 * chunk_flops,
            16,
            {7: 0, 8: 1},
        )
    ahead, back = along(ahead[:middle], 1), along(back[middle:], -1)
    hidden, ahead, back, _, _ = call(
        functools.partial(last_kernel, chips, float(total)),
        (
            jax.ShapeDtypeStruct((held, CORES * units), BF16),
            jax.ShapeDtypeStruct((middle, width), BF16),
            jax.ShapeDtypeStruct((middle, width), BF16),
            *acc_shape,
        ),
        (ahead, back, gains, *weights, acc, square, *downs),
        2 * chunk_flops,
        24,
    )
    for step in range(chips // 2 - 1, 0, -1):
        ahead, back = along(ahead, 1), along(back, -1)
        ahead, back = call(
            functools.partial(down_kernel, chips, step),
            (jax.ShapeDtypeStruct((held, width), BF16),) * 2,
            (hidden, *downs, ahead, back),
            chunk_flops,
            16,
        )
    ahead, back = along(ahead, 1), along(back, -1)
    result = call(
        functools.partial(own_kernel, chips),
        jax.ShapeDtypeStruct((held, width), BF16),
        (hidden, *downs, ahead, back),
        chunk_flops // 2,
        16,
    )
    returned = lax.all_to_all(
        result.reshape(blocks, half, width), "sp", split_axis=0, concat_axis=0, tiled=True
    ).reshape(experts * half, width)
    mine, other = call(
        functools.partial(pick_kernel, experts, capacity),
        (jax.ShapeDtypeStruct((tok_rows, features), F32),) * 2,
        (returned, routes, route_weight),
        4 * experts * half * width * tok_rows,
        12,
    )
    return call(
        join_kernel,
        jax.ShapeDtypeStruct((tok_rows, features), BF16),
        (stored, mine, across(other)),
        tok_rows * features,
        8,
    )


def solution(mesh):
    in_specs = (
        P("sp", "tp"),
        P("tp", None, None),
        P("tp"),
        P(None, "tp"),
        P("sp", "tp"),
        P("tp"),
        P("sp", None),
        P("sp", None),
        P("sp", None, "tp"),
        P("sp", None, "tp"),
        P("sp", "tp", None),
    )
    out_specs = P("sp", "tp")
    return jax.shard_map(
        on_device, mesh=mesh, in_specs=in_specs, out_specs=out_specs, check_vma=False
    )
```

```python
import functools

import jax
import jax.numpy as jnp
from jax import lax
from jax.experimental import pallas as pl
from jax.experimental.pallas import tpu as pltpu
from jax.sharding import PartitionSpec as P


GSIZE = 64
REACH = 16
TOPK = 2
CORES = 2

GATE_LIMIT = 7.0
GATE_ALPHA = 1.702
NORM_EPS = 1e-05

F32 = jnp.float32
BF16 = jnp.bfloat16
MIB = 1024 * 1024


def iota(shape, dim):
    return lax.broadcasted_iota(jnp.int32, shape, dim)


def mm(a, b, ca=1, cb=0):
    return lax.dot_general(a, b, (((ca,), (cb,)), ((), ())), preferred_element_type=F32)


def call(kernel, out_shape, args, flops, mib, aliases=None, space=pltpu.VMEM, scratch=()):
    return pl.pallas_call(
        kernel,
        out_shape=out_shape,
        in_specs=[pl.BlockSpec(memory_space=space)] * len(args),
        scratch_shapes=scratch,
        out_specs=jax.tree.map(lambda _: pl.BlockSpec(memory_space=pltpu.VMEM), out_shape),
        compiler_params=pltpu.CompilerParams(vmem_limit_bytes=mib * MIB),
        cost_estimate=pl.CostEstimate(flops=flops, bytes_accessed=flops // 512, transcendentals=0),
        input_output_aliases=aliases or {},
    )(*args)


def pool_kernel(before_ref, x_ref, w_ref, gain_ref, norm_ref, out_ref):
    rows, width = x_ref.shape
    window = lax.shift_left(jnp.int32(2), lax.rem(lax.axis_index("tp"), 4))
    place = iota((rows, rows), 0) - iota((rows, rows), 1)
    inside = jnp.where((place >= 0) & (place < window), 1.0, 0.0).astype(BF16)
    gap = iota((rows, REACH), 0) + REACH - iota((rows, REACH), 1)
    behind = jnp.where(gap < window, 1.0, 0.0).astype(BF16)
    x = x_ref[...]
    total = mm(inside, x) + mm(behind, before_ref[...])
    spot = lax.axis_index("sp") * rows + iota((rows, 1), 0)
    count = jnp.minimum(spot + 1, window).astype(F32)
    pooled = (total / count - x.astype(F32)).astype(BF16)
    mixed = (mm(pooled, w_ref[...]) * gain_ref[...].astype(F32)).astype(BF16)
    eye = jnp.where(iota((width, width), 0) == iota((width, width), 1), 1.0, 0.0).astype(BF16)
    out_ref[:width, :] = mm(eye, mixed, 1, 1).astype(BF16)
    features = norm_ref.shape[1]
    tail = out_ref.shape[0] - width
    out_ref[width:, :features] = jnp.broadcast_to(norm_ref[...].astype(F32), (tail, features)).astype(BF16)
    out_ref[width:, features:] = jnp.zeros((tail, out_ref.shape[1] - features), BF16)


def row_slots(routes_ref, experts, capacity):
    rows = routes_ref.shape[1]
    named = [iota((experts, rows), 0) == routes_ref[k : k + 1, :] for k in range(TOPK)]
    ones = sum(jnp.where(n, 1.0, 0.0) for n in named)
    upper = jnp.where(iota((rows, rows), 0) < iota((rows, rows), 1), 1.0, 0.0).astype(BF16)
    earlier = mm(ones.astype(BF16), upper)
    slots = []
    for k in range(TOPK):
        rank = jnp.sum(jnp.where(named[k], earlier, 0.0), axis=0, keepdims=True).astype(jnp.int32)
        slots.append(routes_ref[k : k + 1, :] * capacity + rank)
    return slots


def column_slots(routes_ref, experts, capacity):
    rows = routes_ref.shape[0]
    named = [iota((rows, experts), 1) == routes_ref[:, k : k + 1] for k in range(TOPK)]
    ones = sum(jnp.where(n, 1.0, 0.0) for n in named)
    lower = jnp.where(iota((rows, rows), 0) > iota((rows, rows), 1), 1.0, 0.0).astype(BF16)
    earlier = mm(lower, ones.astype(BF16))
    slots = []
    for k in range(TOPK):
        rank = jnp.sum(jnp.where(named[k], earlier, 0.0), axis=1, keepdims=True).astype(jnp.int32)
        slots.append(routes_ref[:, k : k + 1] * capacity + rank)
    return slots


def slot_ids(shape, dim, capacity, core):
    half = capacity // CORES
    place = iota(shape, dim)
    return lax.div(place, half) * capacity + core * half + lax.rem(place, half)


def column_slots(routes_ref, experts, capacity):
    rows = routes_ref.shape[0]
    named = [iota((rows, experts), 1) == routes_ref[:, k : k + 1] for k in range(TOPK)]
    ones = sum(jnp.where(n, 1.0, 0.0) for n in named)
    lower = jnp.where(iota((rows, rows), 0) > iota((rows, rows), 1), 1.0, 0.0).astype(BF16)
    earlier = mm(lower, ones.astype(BF16))
    slots = []
    for k in range(TOPK):
        rank = jnp.sum(jnp.where(named[k], earlier, 0.0), axis=1, keepdims=True).astype(jnp.int32)
        slots.append(routes_ref[:, k : k + 1] * capacity + rank)
    return slots


class Pack:
    def __init__(self, deep, width, channels, rows):
        self.gate, self.up, self.down = 0, deep, 2 * deep
        self.project = 3 * deep
        self.resid = self.project + channels // 2
        self.rows = self.resid + rows // 2
        self.width = width


def prep_kernel(pack, gate, up, down, project, resid, x, w, gain, norm, out, x_out, w_out, gain_out, norm_out, sems):
    width, features = pack.width, project.shape[1]
    units = down.shape[0]
    pairs = [(x, x_out), (w, w_out), (gain, gain_out), (norm, norm_out)]
    for base, source in ((pack.project, project), (pack.resid, resid)):
        half = source.shape[0] // 2
        for i in range(2):
            pairs.append(
                (source.at[i * half : (i + 1) * half, :],
                 out.at[base : base + half, i * features : (i + 1) * features])
            )
    pairs.append((gate, out.at[pack.gate : pack.up, :]))
    pairs.append((up, out.at[pack.up : pack.down, :]))
    for i in range(down.shape[1] // width):
        pairs.append(
            (down.at[:, i * width : (i + 1) * width], out.at[pack.down + i * units : pack.down + (i + 1) * units, :])
        )
    copies = [pltpu.make_async_copy(a, b, sems.at[i]) for i, (a, b) in enumerate(pairs)]
    for copy in copies:
        copy.start()
    for copy in copies:
        copy.wait()


def dispatch_kernel(pack, experts, capacity, mixed_ref, own_ref, other_ref, routes_ref, stream_ref, gain_ref, out_ref):
    core = lax.rem(lax.axis_index("tp"), CORES)
    members, _, rows = mixed_ref.shape
    features = stream_ref.shape[1]
    mixed = mixed_ref[:, :GSIZE, :].reshape(members * GSIZE, rows)
    deep = members * GSIZE // 2
    streams = []
    for ref in (own_ref, other_ref):
        halves = [ref[pack.project : pack.resid, i * features : (i + 1) * features] for i in range(2)]
        projected = mm(mixed[:deep], halves[0], 0, 0) + mm(mixed[deep:], halves[1], 0, 0)
        resid = jnp.concatenate(
            [ref[pack.resid : pack.rows, i * features : (i + 1) * features] for i in range(2)], axis=0
        )
        streams.append((resid.astype(F32) + projected).astype(BF16))
    own, other = streams
    stream_ref[...] = own
    for t in range(members):
        y, c = divmod(t, CORES)
        gain_ref[y, :, c * features : (c + 1) * features] = mixed_ref[t, GSIZE : GSIZE + 8, :features].astype(F32)
    slots = row_slots(routes_ref, experts, capacity)
    ids = slot_ids((out_ref.shape[0], rows), 0, capacity, core)
    hit = (slots[0] == ids) | (slots[1] == ids)
    chosen = jnp.where(hit, 1.0, 0.0).astype(BF16)
    out_ref[:, :features] = mm(chosen, jnp.where(core == 0, own, other)).astype(BF16)
    out_ref[:, features:] = mm(chosen, jnp.where(core == 0, other, own)).astype(BF16)


def add_chunk(pack, x, chip, gain_ref, packs, acc_ref, square_ref, first=False):
    width = x.shape[1]
    value = x.astype(F32)
    square = value * value
    lanes = square_ref.shape[1]
    square = sum(square[:, i : i + lanes] for i in range(0, width, lanes))
    scaled = (value * gain_ref[chip, 0:1, :]).astype(BF16)
    for i, base in enumerate((pack.gate, pack.up)):
        for j, ref in enumerate(packs):
            rows = pl.ds(pl.multiple_of(base + chip * width, width), width)
            part = mm(scaled, ref[rows, :])
            columns = part.shape[1]
            span = slice((2 * i + j) * columns, (2 * i + j + 1) * columns)
            acc_ref[:, span] = part if first else acc_ref[:, span] + part
    square_ref[...] = square if first else square_ref[...] + square


def chip_at(chips, step):
    here = lax.div(lax.axis_index("tp"), CORES)
    return lax.rem(here + step + chips, chips)


def first_kernel(pack, chips, x_ref, gain_ref, own_ref, other_ref, acc_ref, square_ref):
    add_chunk(pack, x_ref[...], chip_at(chips, 0), gain_ref, (own_ref, other_ref), acc_ref, square_ref, True)


def both_kernel(pack, chips, step, p_ref, m_ref, gain_ref, own_ref, other_ref, acc_in, square_in, acc_ref, square_ref):
    packs = (own_ref, other_ref)
    add_chunk(pack, p_ref[...], chip_at(chips, -step), gain_ref, packs, acc_ref, square_ref)
    add_chunk(pack, m_ref[...], chip_at(chips, step), gain_ref, packs, acc_ref, square_ref)


def partial(pack, hidden_ref, packs, chip):
    units = hidden_ref.shape[1] // CORES
    rows = pl.ds(pl.multiple_of(pack.down + chip * units, units), units)
    return sum(mm(hidden_ref[:, i * units : (i + 1) * units], ref[rows, :]) for i, ref in enumerate(packs))


def last_kernel(
    pack, chips, total, p_ref, m_ref, gain_ref, own_ref, other_ref, acc_in, square_in,
    acc_ref, square_ref, hidden_ref, up_ref, low_ref,
):
    x = jnp.concatenate([p_ref[...], m_ref[...]], axis=0)
    packs = (own_ref, other_ref)
    far = chip_at(chips, chips // 2)
    add_chunk(pack, x, far, gain_ref, packs, acc_ref, square_ref)
    mean = jnp.sum(square_ref[...], axis=1, keepdims=True) / total
    scale = lax.rsqrt(mean + NORM_EPS)
    units = hidden_ref.shape[1]
    gate = jnp.minimum(acc_ref[:, :units] * scale, GATE_LIMIT)
    up = jnp.clip(acc_ref[:, units:] * scale, -GATE_LIMIT, GATE_LIMIT)
    hidden_ref[...] = ((up + 1.0) * gate * jax.nn.sigmoid(GATE_ALPHA * gate)).astype(BF16)
    out = partial(pack, hidden_ref, packs, far).astype(BF16)
    half = up_ref.shape[0]
    up_ref[...] = out[:half]
    low_ref[...] = out[half:]


def down_kernel(pack, chips, steps, hidden_ref, own_ref, other_ref, *outs):
    for step, out_ref in zip(steps, outs):
        out_ref[...] = partial(pack, hidden_ref, (own_ref, other_ref), chip_at(chips, step))


def add_kernel(low, part_ref, came_ref, out_ref):
    rows, held = part_ref.shape[0], came_ref.shape[0]
    if held == rows:
        out_ref[...] = (part_ref[...] + came_ref[...].astype(F32)).astype(BF16)
        return
    near = slice(rows - held, rows) if low else slice(0, held)
    rest = slice(0, rows - held) if low else slice(held, rows)
    out_ref[near, :] = (part_ref[near, :] + came_ref[...].astype(F32)).astype(BF16)
    out_ref[rest, :] = part_ref[rest, :].astype(BF16)


def own_kernel(part_ref, p_ref, m_ref, out_ref):
    out_ref[...] = (part_ref[...] + p_ref[...].astype(F32) + m_ref[...].astype(F32)).astype(BF16)


def pick_kernel(experts, capacity, back_ref, routes_ref, weight_ref, mine_ref, other_ref):
    core = lax.rem(lax.axis_index("tp"), CORES)
    slots = column_slots(routes_ref, experts, capacity)
    shape = (routes_ref.shape[0], back_ref.shape[0])
    ids = slot_ids(shape, 1, capacity, core)
    rows = back_ref[...]
    total = 0.0
    for k in range(TOPK):
        chosen = jnp.where(slots[k] == ids, 1.0, 0.0).astype(BF16)
        total = total + mm(chosen, rows) * weight_ref[:, k : k + 1]
    features = mine_ref.shape[1]
    left, right = total[:, :features], total[:, features:]
    mine_ref[...] = jnp.where(core == 0, left, right)
    other_ref[...] = jnp.where(core == 0, right, left)


def join_kernel(stream_ref, mine_ref, other_ref, out_ref):
    out_ref[...] = (stream_ref[...].astype(F32) + mine_ref[...] + other_ref[...]).astype(BF16)


def on_device(
    pool_input,
    pool_weight,
    pool_gain,
    out_weight,
    resid,
    norm_gain,
    routes,
    route_weight,
    expert_gate,
    expert_up,
    expert_down,
):
    tok_rows, channels = pool_input.shape
    features = out_weight.shape[1]
    blocks, members = lax.axis_size("sp"), lax.axis_size("tp")
    chips = members // CORES
    experts = blocks * expert_gate.shape[0]
    capacity = 2 * tok_rows * TOPK // experts
    half = capacity // CORES
    width = features * CORES
    total = features * members
    held = blocks * half

    def along(value, step):
        pairs = [
            (y * CORES + c, (y + step) % chips * CORES + c) for y in range(chips) for c in range(CORES)
        ]
        return lax.ppermute(value, "tp", pairs)

    def across(value):
        return lax.ppermute(value, "tp", [(t, t ^ 1) for t in range(members)])

    shape = jax.ShapeDtypeStruct
    deep, units = expert_gate.shape[1:]
    pack = Pack(deep, width, out_weight.shape[0], tok_rows)
    before = lax.ppermute(
        pool_input[tok_rows - REACH :], "sp", [(s, s + 1) for s in range(blocks - 1)]
    )
    small = (pool_input, pool_weight[0], pool_gain.reshape(1, channels), norm_gain.reshape(1, features))
    own, *small = call(
        functools.partial(prep_kernel, pack),
        (shape((pack.rows, width), BF16), *(shape(v.shape, v.dtype) for v in small)),
        (expert_gate[0], expert_up[0], expert_down[0], out_weight, resid, *small),
        pack.rows * width * 512,
        58,
        space=pltpu.HBM,
        scratch=[pltpu.SemaphoreType.DMA((10 + chips,))],
    )
    other = across(own)
    packs = (own, other)
    pooled = call(
        pool_kernel,
        shape((GSIZE + 16, tok_rows), BF16),
        (before, *small),
        tok_rows * tok_rows * channels * 2,
        8,
    )
    mixed = lax.all_gather(pooled, "tp", axis=0, tiled=False)
    stored, gains, sent = call(
        functools.partial(dispatch_kernel, pack, experts, capacity),
        (
            shape((tok_rows, features), BF16),
            shape((chips, 8, width), F32),
            shape((experts * half, width), BF16),
        ),
        (mixed, *packs, routes.T),
        2 * experts * half * width * tok_rows,
        16,
    )
    x = lax.all_to_all(
        sent.reshape(experts, half, width), "sp", split_axis=0, concat_axis=0, tiled=True
    ).reshape(held, width)

    acc_shape = (shape((held, 4 * units), F32), shape((held, 128), F32))
    chunk_flops = 2 * held * width * 4 * units
    acc, square = call(
        functools.partial(first_kernel, pack, chips), acc_shape, (x, gains, *packs), chunk_flops, 16
    )
    ahead, back = x, x
    middle = held // 2
    last = chips // 2
    for step in range(1, last):
        ahead = along(ahead, 1)
        back = along(back, -1)
        acc, square = call(
            functools.partial(both_kernel, pack, chips, step),
            acc_shape,
            (ahead, back, gains, *packs, acc, square),
            2 * chunk_flops,
            16,
            {5: 0, 6: 1},
        )
    ahead = along(ahead[:middle], 1)
    back = along(back[middle:], -1)
    _, _, hidden, ahead, back = call(
        functools.partial(last_kernel, pack, chips, float(total)),
        (
            *acc_shape,
            shape((held, CORES * units), BF16),
            shape((middle, width), BF16),
            shape((middle, width), BF16),
        ),
        (ahead, back, gains, *packs, acc, square),
        2 * chunk_flops,
        24,
        {5: 0, 6: 1},
    )
    for step in range(last - 1, -1, -1):
        steps = (step, -step) if step else (0,)
        parts = call(
            functools.partial(down_kernel, pack, chips, steps),
            (shape((held, width), F32),) * len(steps),
            (hidden, *packs),
            chunk_flops // 2 * len(steps),
            16,
        )
        ahead = along(ahead, 1)
        back = along(back, -1)
        if step:
            ahead, back = (
                call(
                    functools.partial(add_kernel, low),
                    shape((held, width), BF16),
                    (part, came),
                    held * width,
                    8,
                )
                for low, (part, came) in enumerate(zip(parts, (ahead, back)))
            )
    result = call(own_kernel, shape((held, width), BF16), (*parts, ahead, back), held * width, 8)
    returned = lax.all_to_all(
        result.reshape(blocks, half, width), "sp", split_axis=0, concat_axis=0, tiled=True
    ).reshape(experts * half, width)
    mine, theirs = call(
        functools.partial(pick_kernel, experts, capacity),
        (shape((tok_rows, features), F32),) * 2,
        (returned, routes, route_weight),
        4 * experts * half * width * tok_rows,
        12,
    )
    return call(
        join_kernel,
        shape((tok_rows, features), BF16),
        (stored, mine, across(theirs)),
        tok_rows * features,
        8,
    )


def solution(mesh):
    in_specs = (
        P("sp", "tp"),
        P("tp", None, None),
        P("tp"),
        P(None, "tp"),
        P("sp", "tp"),
        P("tp"),
        P("sp", None),
        P("sp", None),
        P("sp", None, "tp"),
        P("sp", None, "tp"),
        P("sp", "tp", None),
    )
    out_specs = P("sp", "tp")

    return jax.shard_map(on_device, mesh=mesh, in_specs=in_specs, out_specs=out_specs, check_vma=False)
```

```python
import functools

import jax
import jax.numpy as jnp
from jax import lax
from jax.experimental import pallas as pl
from jax.experimental.pallas import tpu as pltpu
from jax.sharding import PartitionSpec as P


GSIZE = 64
REACH = 16
TOPK = 2
CORES = 2

GATE_LIMIT = 7.0
GATE_ALPHA = 1.702
NORM_EPS = 1e-05

F32 = jnp.float32
BF16 = jnp.bfloat16
MIB = 1024 * 1024


def iota(shape, dim):
    return lax.broadcasted_iota(jnp.int32, shape, dim)


def mm(a, b, ca=1, cb=0):
    return lax.dot_general(a, b, (((ca,), (cb,)), ((), ())), preferred_element_type=F32)


def call(kernel, out_shape, args, flops, mib, aliases=None, space=pltpu.VMEM, scratch=()):
    return pl.pallas_call(
        kernel,
        out_shape=out_shape,
        in_specs=[pl.BlockSpec(memory_space=space)] * len(args),
        scratch_shapes=scratch,
        out_specs=jax.tree.map(lambda _: pl.BlockSpec(memory_space=pltpu.VMEM), out_shape),
        compiler_params=pltpu.CompilerParams(vmem_limit_bytes=mib * MIB),
        cost_estimate=pl.CostEstimate(flops=flops, bytes_accessed=flops // 512, transcendentals=0),
        input_output_aliases=aliases or {},
    )(*args)


def pool_kernel(before_ref, x_ref, w_ref, gain_ref, norm_ref, out_ref):
    width, rows = x_ref.shape
    window = lax.shift_left(jnp.int32(2), lax.rem(lax.axis_index("tp"), 4))
    place = iota((rows, rows), 1) - iota((rows, rows), 0)
    inside = jnp.where((place >= 0) & (place < window), 1.0, 0.0).astype(BF16)
    reach = before_ref.shape[1]
    gap = iota((reach, rows), 1) + reach - iota((reach, rows), 0)
    behind = jnp.where(gap < window, 1.0, 0.0).astype(BF16)
    x = x_ref[...]
    total = mm(x, inside) + mm(before_ref[...], behind)
    spot = lax.axis_index("sp") * rows + iota((1, rows), 1)
    count = jnp.minimum(spot + 1, window).astype(F32)
    pooled = (total / count - x.astype(F32)).astype(BF16)
    eye = iota((width, width), 0) == iota((width, width), 1)
    gain = jnp.sum(jnp.where(eye, gain_ref[...].astype(F32), 0.0), axis=1, keepdims=True)
    out_ref[:width, :] = (mm(w_ref[...], pooled, 0, 0) * gain).astype(BF16)
    features = norm_ref.shape[1]
    tail = out_ref.shape[0] - width
    out_ref[width:, :features] = jnp.broadcast_to(norm_ref[...].astype(F32), (tail, features)).astype(BF16)
    out_ref[width:, features:] = jnp.zeros((tail, out_ref.shape[1] - features), BF16)


def row_slots(routes_ref, experts, capacity):
    rows = routes_ref.shape[1]
    named = [iota((experts, rows), 0) == routes_ref[k : k + 1, :] for k in range(TOPK)]
    ones = sum(jnp.where(n, 1.0, 0.0) for n in named)
    upper = jnp.where(iota((rows, rows), 0) < iota((rows, rows), 1), 1.0, 0.0).astype(BF16)
    earlier = mm(ones.astype(BF16), upper)
    slots = []
    for k in range(TOPK):
        rank = jnp.sum(jnp.where(named[k], earlier, 0.0), axis=0, keepdims=True).astype(jnp.int32)
        slots.append(routes_ref[k : k + 1, :] * capacity + rank)
    return slots


def column_slots(routes_ref, experts, capacity):
    rows = routes_ref.shape[0]
    named = [iota((rows, experts), 1) == routes_ref[:, k : k + 1] for k in range(TOPK)]
    ones = sum(jnp.where(n, 1.0, 0.0) for n in named)
    lower = jnp.where(iota((rows, rows), 0) > iota((rows, rows), 1), 1.0, 0.0).astype(BF16)
    earlier = mm(lower, ones.astype(BF16))
    slots = []
    for k in range(TOPK):
        rank = jnp.sum(jnp.where(named[k], earlier, 0.0), axis=1, keepdims=True).astype(jnp.int32)
        slots.append(routes_ref[:, k : k + 1] * capacity + rank)
    return slots


def slot_ids(shape, dim, capacity, core):
    half = capacity // CORES
    place = iota(shape, dim)
    return lax.div(place, half) * capacity + core * half + lax.rem(place, half)


def column_slots(routes_ref, experts, capacity):
    rows = routes_ref.shape[0]
    named = [iota((rows, experts), 1) == routes_ref[:, k : k + 1] for k in range(TOPK)]
    ones = sum(jnp.where(n, 1.0, 0.0) for n in named)
    lower = jnp.where(iota((rows, rows), 0) > iota((rows, rows), 1), 1.0, 0.0).astype(BF16)
    earlier = mm(lower, ones.astype(BF16))
    slots = []
    for k in range(TOPK):
        rank = jnp.sum(jnp.where(named[k], earlier, 0.0), axis=1, keepdims=True).astype(jnp.int32)
        slots.append(routes_ref[:, k : k + 1] * capacity + rank)
    return slots


class Pack:
    def __init__(self, deep, width, channels, rows):
        self.gate, self.up, self.down = 0, deep, 2 * deep
        self.project = 3 * deep
        self.resid = self.project + channels // 2
        self.rows = self.resid + rows // 2
        self.width = width


def prep_kernel(pack, gate, up, down, project, resid, x, w, gain, norm, out, x_out, w_out, gain_out, norm_out, sems):
    width, features = pack.width, project.shape[1]
    units = down.shape[0]
    pairs = [(x, x_out), (w, w_out), (gain, gain_out), (norm, norm_out)]
    for base, source in ((pack.project, project), (pack.resid, resid)):
        half = source.shape[0] // 2
        for i in range(2):
            pairs.append(
                (source.at[i * half : (i + 1) * half, :],
                 out.at[base : base + half, i * features : (i + 1) * features])
            )
    pairs.append((gate, out.at[pack.gate : pack.up, :]))
    pairs.append((up, out.at[pack.up : pack.down, :]))
    for i in range(down.shape[1] // width):
        pairs.append(
            (down.at[:, i * width : (i + 1) * width], out.at[pack.down + i * units : pack.down + (i + 1) * units, :])
        )
    copies = [pltpu.make_async_copy(a, b, sems.at[i]) for i, (a, b) in enumerate(pairs)]
    for copy in copies:
        copy.start()
    for copy in copies:
        copy.wait()


def dispatch_kernel(pack, experts, capacity, mixed_ref, own_ref, other_ref, routes_ref, stream_ref, gain_ref, out_ref):
    core = lax.rem(lax.axis_index("tp"), CORES)
    members, _, rows = mixed_ref.shape
    features = stream_ref.shape[1]
    mixed = mixed_ref[:, :GSIZE, :].reshape(members * GSIZE, rows)
    deep = members * GSIZE // 2
    streams = []
    for ref in (own_ref, other_ref):
        halves = [ref[pack.project : pack.resid, i * features : (i + 1) * features] for i in range(2)]
        projected = mm(mixed[:deep], halves[0], 0, 0) + mm(mixed[deep:], halves[1], 0, 0)
        resid = jnp.concatenate(
            [ref[pack.resid : pack.rows, i * features : (i + 1) * features] for i in range(2)], axis=0
        )
        streams.append((resid.astype(F32) + projected).astype(BF16))
    own, other = streams
    stream_ref[...] = own
    for t in range(members):
        y, c = divmod(t, CORES)
        gain_ref[y, :, c * features : (c + 1) * features] = mixed_ref[t, GSIZE : GSIZE + 8, :features].astype(F32)
    slots = row_slots(routes_ref, experts, capacity)
    ids = slot_ids((out_ref.shape[0], rows), 0, capacity, core)
    hit = (slots[0] == ids) | (slots[1] == ids)
    chosen = jnp.where(hit, 1.0, 0.0).astype(BF16)
    out_ref[:, :features] = mm(chosen, jnp.where(core == 0, own, other)).astype(BF16)
    out_ref[:, features:] = mm(chosen, jnp.where(core == 0, other, own)).astype(BF16)


def add_chunk(pack, x, chip, gain_ref, packs, acc_ref, square_ref, first=False):
    width = x.shape[1]
    value = x.astype(F32)
    square = value * value
    lanes = square_ref.shape[1]
    square = sum(square[:, i : i + lanes] for i in range(0, width, lanes))
    scaled = (value * gain_ref[chip, 0:1, :]).astype(BF16)
    for i, base in enumerate((pack.gate, pack.up)):
        for j, ref in enumerate(packs):
            rows = pl.ds(pl.multiple_of(base + chip * width, width), width)
            part = mm(scaled, ref[rows, :])
            columns = part.shape[1]
            span = slice((2 * i + j) * columns, (2 * i + j + 1) * columns)
            acc_ref[:, span] = part if first else acc_ref[:, span] + part
    square_ref[...] = square if first else square_ref[...] + square


def chip_at(chips, step):
    here = lax.div(lax.axis_index("tp"), CORES)
    return lax.rem(here + step + chips, chips)


def first_kernel(pack, chips, x_ref, gain_ref, own_ref, other_ref, acc_ref, square_ref):
    add_chunk(pack, x_ref[...], chip_at(chips, 0), gain_ref, (own_ref, other_ref), acc_ref, square_ref, True)


def both_kernel(pack, chips, step, p_ref, m_ref, gain_ref, own_ref, other_ref, acc_in, square_in, acc_ref, square_ref):
    packs = (own_ref, other_ref)
    add_chunk(pack, p_ref[...], chip_at(chips, -step), gain_ref, packs, acc_ref, square_ref)
    add_chunk(pack, m_ref[...], chip_at(chips, step), gain_ref, packs, acc_ref, square_ref)


def partial(pack, hidden_ref, packs, chip):
    units = hidden_ref.shape[1] // CORES
    rows = pl.ds(pl.multiple_of(pack.down + chip * units, units), units)
    return sum(mm(hidden_ref[:, i * units : (i + 1) * units], ref[rows, :]) for i, ref in enumerate(packs))


def last_kernel(
    pack, chips, total, p_ref, gain_ref, own_ref, other_ref, acc_in, square_in, acc_ref, square_ref, hidden_ref, out_ref
):
    packs = (own_ref, other_ref)
    far = chip_at(chips, chips // 2)
    add_chunk(pack, p_ref[...], far, gain_ref, packs, acc_ref, square_ref)
    mean = jnp.sum(square_ref[...], axis=1, keepdims=True) / total
    scale = lax.rsqrt(mean + NORM_EPS)
    units = hidden_ref.shape[1]
    gate = jnp.minimum(acc_ref[:, :units] * scale, GATE_LIMIT)
    up = jnp.clip(acc_ref[:, units:] * scale, -GATE_LIMIT, GATE_LIMIT)
    hidden_ref[...] = ((up + 1.0) * gate * jax.nn.sigmoid(GATE_ALPHA * gate)).astype(BF16)
    out_ref[...] = partial(pack, hidden_ref, packs, far).astype(BF16)


def down_kernel(pack, chips, steps, hidden_ref, own_ref, other_ref, *outs):
    for step, out_ref in zip(steps, outs):
        value = partial(pack, hidden_ref, (own_ref, other_ref), chip_at(chips, step))
        out_ref[...] = value.astype(out_ref.dtype)


def add_kernel(part_ref, came_ref, out_ref):
    out_ref[...] = (part_ref[...] + came_ref[...].astype(F32)).astype(BF16)


def own_kernel(part_ref, p_ref, m_ref, out_ref):
    out_ref[...] = (part_ref[...] + p_ref[...].astype(F32) + m_ref[...].astype(F32)).astype(BF16)


def pick_kernel(experts, capacity, back_ref, routes_ref, weight_ref, mine_ref, other_ref):
    core = lax.rem(lax.axis_index("tp"), CORES)
    slots = column_slots(routes_ref, experts, capacity)
    shape = (routes_ref.shape[0], back_ref.shape[0])
    ids = slot_ids(shape, 1, capacity, core)
    rows = back_ref[...]
    total = 0.0
    for k in range(TOPK):
        chosen = jnp.where(slots[k] == ids, 1.0, 0.0).astype(BF16)
        total = total + mm(chosen, rows) * weight_ref[:, k : k + 1]
    features = mine_ref.shape[1]
    left, right = total[:, :features], total[:, features:]
    mine_ref[...] = jnp.where(core == 0, left, right)
    other_ref[...] = jnp.where(core == 0, right, left)


def join_kernel(stream_ref, mine_ref, other_ref, out_ref):
    out_ref[...] = (stream_ref[...].astype(F32) + mine_ref[...] + other_ref[...]).astype(BF16)


def on_device(
    pool_input,
    pool_weight,
    pool_gain,
    out_weight,
    resid,
    norm_gain,
    routes,
    route_weight,
    expert_gate,
    expert_up,
    expert_down,
):
    tok_rows, channels = pool_input.shape
    features = out_weight.shape[1]
    blocks, members = lax.axis_size("sp"), lax.axis_size("tp")
    chips = members // CORES
    experts = blocks * expert_gate.shape[0]
    capacity = 2 * tok_rows * TOPK // experts
    half = capacity // CORES
    width = features * CORES
    total = features * members
    held = blocks * half

    def along(value, step):
        pairs = [
            (y * CORES + c, (y + step) % chips * CORES + c) for y in range(chips) for c in range(CORES)
        ]
        return lax.ppermute(value, "tp", pairs)

    def across(value):
        return lax.ppermute(value, "tp", [(t, t ^ 1) for t in range(members)])

    shape = jax.ShapeDtypeStruct
    deep, units = expert_gate.shape[1:]
    pack = Pack(deep, width, out_weight.shape[0], tok_rows)
    before = lax.ppermute(
        pool_input.T[:, tok_rows - REACH * 8 :], "sp", [(s, s + 1) for s in range(blocks - 1)]
    )
    small = (pool_input.T, pool_weight[0], pool_gain.reshape(1, channels), norm_gain.reshape(1, features))
    own, *small = call(
        functools.partial(prep_kernel, pack),
        (pltpu.VMEM((pack.rows, width), BF16), *(pltpu.VMEM(v.shape, v.dtype) for v in small)),
        tuple(
            pltpu.with_memory_space_constraint(v, pltpu.HBM)
            for v in (expert_gate[0], expert_up[0], expert_down[0], out_weight, resid, *small)
        ),
        pack.rows * width * 512,
        8,
        space=pltpu.HBM,
        scratch=[pltpu.SemaphoreType.DMA((10 + chips,))],
    )
    other = across(own)
    packs = (own, other)
    pooled = call(
        pool_kernel,
        shape((GSIZE + 16, tok_rows), BF16),
        (before, *small),
        tok_rows * tok_rows * channels * 2,
        8,
    )
    mixed = lax.all_gather(pooled, "tp", axis=0, tiled=False)
    stored, gains, sent = call(
        functools.partial(dispatch_kernel, pack, experts, capacity),
        (
            shape((tok_rows, features), BF16),
            shape((chips, 8, width), F32),
            shape((experts * half, width), BF16),
        ),
        (mixed, *packs, routes.T),
        2 * experts * half * width * tok_rows,
        16,
    )
    x = lax.all_to_all(
        sent.reshape(experts, half, width), "sp", split_axis=0, concat_axis=0, tiled=True
    ).reshape(held, width)

    acc_shape = (shape((held, 4 * units), F32), shape((held, 128), F32))
    chunk_flops = 2 * held * width * 4 * units
    acc, square = call(
        functools.partial(first_kernel, pack, chips), acc_shape, (x, gains, *packs), chunk_flops, 16
    )
    ahead, back = x, x
    last = chips // 2
    for step in range(1, last):
        ahead = along(ahead, 1)
        back = along(back, -1)
        acc, square = call(
            functools.partial(both_kernel, pack, chips, step),
            acc_shape,
            (ahead, back, gains, *packs, acc, square),
            2 * chunk_flops,
            16,
            {5: 0, 6: 1},
        )
    ahead = along(ahead, 1)
    _, _, hidden, ahead = call(
        functools.partial(last_kernel, pack, chips, float(total)),
        (*acc_shape, shape((held, CORES * units), BF16), shape((held, width), BF16)),
        (ahead, gains, *packs, acc, square),
        2 * chunk_flops,
        24,
        {4: 0, 5: 1},
    )

    def joined(part, came):
        return call(add_kernel, shape((held, width), BF16), (part, came), held * width, 8)

    for step in range(last - 1, -1, -1):
        ahead = along(ahead, 1)
        steps = (step, -step) if step else (0,)
        kinds = (F32, BF16 if step == last - 1 else F32)[: len(steps)]
        parts = call(
            functools.partial(down_kernel, pack, chips, steps),
            tuple(shape((held, width), kind) for kind in kinds),
            (hidden, *packs),
            chunk_flops // 2 * len(steps),
            16,
        )
        if step == last - 1:
            back = parts[1]
        else:
            back = along(back, -1)
            back = joined(parts[1], back) if step else back
        ahead = joined(parts[0], ahead) if step else ahead
    result = call(own_kernel, shape((held, width), BF16), (*parts, ahead, back), held * width, 8)
    returned = lax.all_to_all(
        result.reshape(blocks, half, width), "sp", split_axis=0, concat_axis=0, tiled=True
    ).reshape(experts * half, width)
    mine, theirs = call(
        functools.partial(pick_kernel, experts, capacity),
        (shape((tok_rows, features), F32),) * 2,
        (returned, routes, route_weight),
        4 * experts * half * width * tok_rows,
        12,
    )
    return call(
        join_kernel,
        shape((tok_rows, features), BF16),
        (stored, mine, across(theirs)),
        tok_rows * features,
        8,
    )


def solution(mesh):
    in_specs = (
        P("sp", "tp"),
        P("tp", None, None),
        P("tp"),
        P(None, "tp"),
        P("sp", "tp"),
        P("tp"),
        P("sp", None),
        P("sp", None),
        P("sp", None, "tp"),
        P("sp", None, "tp"),
        P("sp", "tp", None),
    )
    out_specs = P("sp", "tp")

    return jax.shard_map(on_device, mesh=mesh, in_specs=in_specs, out_specs=out_specs, check_vma=False)
```

```python
import functools

import jax
import jax.numpy as jnp
from jax import lax
from jax.experimental import pallas as pl
from jax.experimental.pallas import tpu as pltpu
from jax.sharding import PartitionSpec as P


GSIZE = 64
TOPK = 2
CORES = 2

GATE_LIMIT = 7.0
GATE_ALPHA = 1.702
NORM_EPS = 1e-05

F32 = jnp.float32
BF16 = jnp.bfloat16
MIB = 1024 * 1024


def iota(shape, dim):
    return lax.broadcasted_iota(jnp.int32, shape, dim)


def mm(a, b, ca=1, cb=0):
    return lax.dot_general(a, b, (((ca,), (cb,)), ((), ())), preferred_element_type=F32)


def call(kernel, out_shape, args, flops, mib, aliases=None, space=pltpu.VMEM, scratch=()):
    return pl.pallas_call(
        kernel,
        out_shape=out_shape,
        in_specs=[pl.BlockSpec(memory_space=space)] * len(args),
        scratch_shapes=scratch,
        out_specs=jax.tree.map(lambda _: pl.BlockSpec(memory_space=pltpu.VMEM), out_shape),
        compiler_params=pltpu.CompilerParams(vmem_limit_bytes=mib * MIB),
        cost_estimate=pl.CostEstimate(flops=flops, bytes_accessed=flops // 512, transcendentals=0),
        input_output_aliases=aliases or {},
    )(*args)


def pool_kernel(before_ref, x_ref, w_ref, gain_ref, norm_ref, out_ref):
    width, rows = x_ref.shape
    window = lax.shift_left(jnp.int32(2), lax.rem(lax.axis_index("tp"), 4))
    place = iota((rows, rows), 1) - iota((rows, rows), 0)
    inside = jnp.where((place >= 0) & (place < window), 1.0, 0.0).astype(BF16)
    reach = before_ref.shape[1]
    gap = iota((reach, rows), 1) + reach - iota((reach, rows), 0)
    behind = jnp.where(gap < window, 1.0, 0.0).astype(BF16)
    x = x_ref[...]
    total = mm(x, inside) + mm(before_ref[...], behind)
    spot = lax.axis_index("sp") * rows + iota((1, rows), 1)
    count = jnp.minimum(spot + 1, window).astype(F32)
    pooled = (total / count - x.astype(F32)).astype(BF16)
    eye = iota((width, width), 0) == iota((width, width), 1)
    gain = jnp.sum(jnp.where(eye, gain_ref[...].astype(F32), 0.0), axis=1, keepdims=True)
    out_ref[:width, :] = (mm(w_ref[...], pooled, 0, 0) * gain).astype(BF16)
    features = norm_ref.shape[1]
    tail = out_ref.shape[0] - width
    out_ref[width:, :features] = jnp.broadcast_to(norm_ref[...].astype(F32), (tail, features)).astype(BF16)
    out_ref[width:, features:] = jnp.zeros((tail, out_ref.shape[1] - features), BF16)


def row_slots(routes_ref, experts, capacity):
    rows = routes_ref.shape[1]
    named = [iota((experts, rows), 0) == routes_ref[k : k + 1, :] for k in range(TOPK)]
    ones = sum(jnp.where(n, 1.0, 0.0) for n in named)
    upper = jnp.where(iota((rows, rows), 0) < iota((rows, rows), 1), 1.0, 0.0).astype(BF16)
    earlier = mm(ones.astype(BF16), upper)
    slots = []
    for k in range(TOPK):
        rank = jnp.sum(jnp.where(named[k], earlier, 0.0), axis=0, keepdims=True).astype(jnp.int32)
        slots.append(routes_ref[k : k + 1, :] * capacity + rank)
    return slots


def column_slots(routes_ref, experts, capacity):
    rows = routes_ref.shape[0]
    named = [iota((rows, experts), 1) == routes_ref[:, k : k + 1] for k in range(TOPK)]
    ones = sum(jnp.where(n, 1.0, 0.0) for n in named)
    lower = jnp.where(iota((rows, rows), 0) > iota((rows, rows), 1), 1.0, 0.0).astype(BF16)
    earlier = mm(lower, ones.astype(BF16))
    slots = []
    for k in range(TOPK):
        rank = jnp.sum(jnp.where(named[k], earlier, 0.0), axis=1, keepdims=True).astype(jnp.int32)
        slots.append(routes_ref[:, k : k + 1] * capacity + rank)
    return slots


def slot_ids(shape, dim, capacity, core):
    half = capacity // CORES
    place = iota(shape, dim)
    return lax.div(place, half) * capacity + core * half + lax.rem(place, half)


def column_slots(routes_ref, experts, capacity):
    rows = routes_ref.shape[0]
    named = [iota((rows, experts), 1) == routes_ref[:, k : k + 1] for k in range(TOPK)]
    ones = sum(jnp.where(n, 1.0, 0.0) for n in named)
    lower = jnp.where(iota((rows, rows), 0) > iota((rows, rows), 1), 1.0, 0.0).astype(BF16)
    earlier = mm(lower, ones.astype(BF16))
    slots = []
    for k in range(TOPK):
        rank = jnp.sum(jnp.where(named[k], earlier, 0.0), axis=1, keepdims=True).astype(jnp.int32)
        slots.append(routes_ref[:, k : k + 1] * capacity + rank)
    return slots


class Pack:
    def __init__(self, deep, width, channels, rows):
        self.gate, self.up, self.down = 0, deep, 2 * deep
        self.project = 3 * deep
        self.resid = self.project + channels // 2
        self.rows = self.resid + rows // 2
        self.width = width


def prep_kernel(pack, gate, up, down, project, resid, x, w, gain, norm, out, x_out, w_out, gain_out, norm_out, sems):
    width, features = pack.width, project.shape[1]
    units = down.shape[0]
    pairs = [(x, x_out), (w, w_out), (gain, gain_out), (norm, norm_out)]
    for base, source in ((pack.project, project), (pack.resid, resid)):
        half = source.shape[0] // 2
        for i in range(2):
            pairs.append(
                (source.at[i * half : (i + 1) * half, :],
                 out.at[base : base + half, i * features : (i + 1) * features])
            )
    pairs.append((gate, out.at[pack.gate : pack.up, :]))
    pairs.append((up, out.at[pack.up : pack.down, :]))
    for i in range(down.shape[1] // width):
        pairs.append(
            (down.at[:, i * width : (i + 1) * width], out.at[pack.down + i * units : pack.down + (i + 1) * units, :])
        )
    copies = [pltpu.make_async_copy(a, b, sems.at[i]) for i, (a, b) in enumerate(pairs)]
    for copy in copies:
        copy.start()
    for copy in copies:
        copy.wait()


def dispatch_kernel(pack, experts, capacity, mixed_ref, own_ref, other_ref, routes_ref, stream_ref, gain_ref, out_ref):
    core = lax.rem(lax.axis_index("tp"), CORES)
    members, _, rows = mixed_ref.shape
    features = stream_ref.shape[1]
    mixed = mixed_ref[:, :GSIZE, :].reshape(members * GSIZE, rows)
    deep = members * GSIZE // 2
    streams = []
    for ref in (own_ref, other_ref):
        halves = [ref[pack.project : pack.resid, i * features : (i + 1) * features] for i in range(2)]
        projected = mm(mixed[:deep], halves[0], 0, 0) + mm(mixed[deep:], halves[1], 0, 0)
        resid = jnp.concatenate(
            [ref[pack.resid : pack.rows, i * features : (i + 1) * features] for i in range(2)], axis=0
        )
        streams.append((resid.astype(F32) + projected).astype(BF16))
    own, other = streams
    stream_ref[...] = own
    for t in range(members):
        y, c = divmod(t, CORES)
        gain_ref[y, :, c * features : (c + 1) * features] = mixed_ref[t, GSIZE : GSIZE + 8, :features].astype(F32)
    slots = row_slots(routes_ref, experts, capacity)
    ids = slot_ids((out_ref.shape[0], rows), 0, capacity, core)
    hit = (slots[0] == ids) | (slots[1] == ids)
    chosen = jnp.where(hit, 1.0, 0.0).astype(BF16)
    out_ref[:, :features] = mm(chosen, jnp.where(core == 0, own, other)).astype(BF16)
    out_ref[:, features:] = mm(chosen, jnp.where(core == 0, other, own)).astype(BF16)


def add_chunk(pack, x, chip, gain_ref, packs, acc_ref, square_ref, first=False):
    width = x.shape[1]
    value = x.astype(F32)
    square = value * value
    lanes = square_ref.shape[1]
    square = sum(square[:, i : i + lanes] for i in range(0, width, lanes))
    scaled = (value * gain_ref[chip, 0:1, :]).astype(BF16)
    for i, base in enumerate((pack.gate, pack.up)):
        for j, ref in enumerate(packs):
            rows = pl.ds(pl.multiple_of(base + chip * width, width), width)
            part = mm(scaled, ref[rows, :])
            columns = part.shape[1]
            span = slice((2 * i + j) * columns, (2 * i + j + 1) * columns)
            acc_ref[:, span] = part if first else acc_ref[:, span] + part
    square_ref[...] = square if first else square_ref[...] + square


def chip_at(chips, step):
    here = lax.div(lax.axis_index("tp"), CORES)
    return lax.rem(here + step + chips, chips)


def first_kernel(pack, chips, x_ref, gain_ref, own_ref, other_ref, acc_ref, square_ref):
    add_chunk(pack, x_ref[...], chip_at(chips, 0), gain_ref, (own_ref, other_ref), acc_ref, square_ref, True)


def both_kernel(pack, chips, step, p_ref, m_ref, gain_ref, own_ref, other_ref, acc_in, square_in, acc_ref, square_ref):
    packs = (own_ref, other_ref)
    add_chunk(pack, p_ref[...], chip_at(chips, -step), gain_ref, packs, acc_ref, square_ref)
    add_chunk(pack, m_ref[...], chip_at(chips, step), gain_ref, packs, acc_ref, square_ref)


def partial(pack, hidden_ref, packs, chip):
    units = hidden_ref.shape[1] // CORES
    rows = pl.ds(pl.multiple_of(pack.down + chip * units, units), units)
    return sum(mm(hidden_ref[:, i * units : (i + 1) * units], ref[rows, :]) for i, ref in enumerate(packs))


def last_kernel(
    pack, chips, total, p_ref, gain_ref, own_ref, other_ref, acc_in, square_in, acc_ref, square_ref, hidden_ref, up_ref, low_ref
):
    packs = (own_ref, other_ref)
    far = chip_at(chips, chips // 2)
    add_chunk(pack, p_ref[...], far, gain_ref, packs, acc_ref, square_ref)
    mean = jnp.sum(square_ref[...], axis=1, keepdims=True) / total
    scale = lax.rsqrt(mean + NORM_EPS)
    units = hidden_ref.shape[1]
    gate = jnp.minimum(acc_ref[:, :units] * scale, GATE_LIMIT)
    up = jnp.clip(acc_ref[:, units:] * scale, -GATE_LIMIT, GATE_LIMIT)
    hidden_ref[...] = ((up + 1.0) * gate * jax.nn.sigmoid(GATE_ALPHA * gate)).astype(BF16)
    up_ref[...] = partial(pack, hidden_ref, packs, far).astype(BF16)
    low_ref[...] = partial(pack, hidden_ref, packs, chip_at(chips, 1 - chips // 2)).astype(BF16)


def down_kernel(pack, chips, steps, hidden_ref, own_ref, other_ref, *outs):
    for step, out_ref in zip(steps, outs):
        out_ref[...] = partial(pack, hidden_ref, (own_ref, other_ref), chip_at(chips, step))


def add_kernel(part_ref, came_ref, out_ref):
    out_ref[...] = (part_ref[...] + came_ref[...].astype(F32)).astype(BF16)


def own_kernel(part_ref, p_ref, m_ref, out_ref):
    out_ref[...] = (part_ref[...] + p_ref[...].astype(F32) + m_ref[...].astype(F32)).astype(BF16)


def pick_kernel(experts, capacity, back_ref, routes_ref, weight_ref, mine_ref, other_ref):
    core = lax.rem(lax.axis_index("tp"), CORES)
    slots = column_slots(routes_ref, experts, capacity)
    shape = (routes_ref.shape[0], back_ref.shape[0])
    ids = slot_ids(shape, 1, capacity, core)
    rows = back_ref[...]
    total = 0.0
    for k in range(TOPK):
        chosen = jnp.where(slots[k] == ids, 1.0, 0.0).astype(BF16)
        total = total + mm(chosen, rows) * weight_ref[:, k : k + 1]
    features = mine_ref.shape[1]
    left, right = total[:, :features], total[:, features:]
    mine_ref[...] = jnp.where(core == 0, left, right)
    other_ref[...] = jnp.where(core == 0, right, left)


def join_kernel(stream_ref, mine_ref, other_ref, out_ref):
    out_ref[...] = (stream_ref[...].astype(F32) + mine_ref[...] + other_ref[...]).astype(BF16)


def on_device(
    pool_input,
    pool_weight,
    pool_gain,
    out_weight,
    resid,
    norm_gain,
    routes,
    route_weight,
    expert_gate,
    expert_up,
    expert_down,
):
    tok_rows, channels = pool_input.shape
    features = out_weight.shape[1]
    blocks, members = lax.axis_size("sp"), lax.axis_size("tp")
    chips = members // CORES
    experts = blocks * expert_gate.shape[0]
    capacity = 2 * tok_rows * TOPK // experts
    half = capacity // CORES
    width = features * CORES
    total = features * members
    held = blocks * half

    def along(value, step):
        pairs = [
            (y * CORES + c, (y + step) % chips * CORES + c) for y in range(chips) for c in range(CORES)
        ]
        return lax.ppermute(value, "tp", pairs)

    def across(value):
        return lax.ppermute(value, "tp", [(t, t ^ 1) for t in range(members)])

    shape = jax.ShapeDtypeStruct
    deep, units = expert_gate.shape[1:]
    pack = Pack(deep, width, out_weight.shape[0], tok_rows)
    before = lax.ppermute(
        pool_input.T, "sp", [(s, s + 1) for s in range(blocks - 1)]
    )
    small = (pool_input.T, pool_weight[0], pool_gain.reshape(1, channels), norm_gain.reshape(1, features))
    own, *small = call(
        functools.partial(prep_kernel, pack),
        (pltpu.VMEM((pack.rows, width), BF16), *(pltpu.VMEM(v.shape, v.dtype) for v in small)),
        tuple(
            pltpu.with_memory_space_constraint(v, pltpu.HBM)
            for v in (expert_gate[0], expert_up[0], expert_down[0], out_weight, resid, *small)
        ),
        pack.rows * width * 512,
        8,
        space=pltpu.HBM,
        scratch=[pltpu.SemaphoreType.DMA((10 + chips,))],
    )
    other = across(own)
    packs = (own, other)
    pooled = call(
        pool_kernel,
        shape((GSIZE + 16, tok_rows), BF16),
        (before, *small),
        tok_rows * tok_rows * channels * 2,
        8,
    )
    mixed = lax.all_gather(pooled, "tp", axis=0, tiled=False)
    stored, gains, sent = call(
        functools.partial(dispatch_kernel, pack, experts, capacity),
        (
            shape((tok_rows, features), BF16),
            shape((chips, 8, width), F32),
            shape((experts * half, width), BF16),
        ),
        (mixed, *packs, routes.T),
        2 * experts * half * width * tok_rows,
        16,
    )
    x = lax.all_to_all(
        sent.reshape(experts, half, width), "sp", split_axis=0, concat_axis=0, tiled=True
    ).reshape(held, width)

    acc_shape = (shape((held, 4 * units), F32), shape((held, 128), F32))
    chunk_flops = 2 * held * width * 4 * units
    acc, square = call(
        functools.partial(first_kernel, pack, chips), acc_shape, (x, gains, *packs), chunk_flops, 16
    )
    ahead, back = x, x
    last = chips // 2
    for step in range(1, last):
        ahead = along(ahead, 1)
        back = along(back, -1)
        acc, square = call(
            functools.partial(both_kernel, pack, chips, step),
            acc_shape,
            (ahead, back, gains, *packs, acc, square),
            2 * chunk_flops,
            16,
            {5: 0, 6: 1},
        )
    ahead = along(ahead, 1)
    _, _, hidden, ahead, back = call(
        functools.partial(last_kernel, pack, chips, float(total)),
        (*acc_shape, shape((held, CORES * units), BF16), *(shape((held, width), BF16),) * 2),
        (ahead, gains, *packs, acc, square),
        2 * chunk_flops,
        24,
        {4: 0, 5: 1},
    )

    def joined(part, came):
        return call(add_kernel, shape((held, width), BF16), (part, came), held * width, 8)

    steps = [*range(last - 1, -1, -1), *range(2 - last, 0)]
    parts = call(
        functools.partial(down_kernel, pack, chips, steps),
        (shape((held, width), F32),) * len(steps),
        (hidden, *packs),
        chunk_flops // 2 * len(steps),
        24,
    )
    part = dict(zip(steps, parts))
    for step in range(last - 1, -1, -1):
        ahead = along(ahead, 1)
        if step:
            back = along(back, -1)
            ahead = joined(part[step], ahead)
            back = joined(part[1 - step], back) if step > 1 else back
    result = call(own_kernel, pltpu.VMEM((held, width), BF16), (part[0], ahead, back), held * width, 8)
    returned = lax.all_to_all(
        result.reshape(blocks, half, width), "sp", split_axis=0, concat_axis=0, tiled=True
    ).reshape(experts * half, width)
    mine, theirs = call(
        functools.partial(pick_kernel, experts, capacity),
        (shape((tok_rows, features), F32),) * 2,
        (returned, routes, route_weight),
        4 * experts * half * width * tok_rows,
        12,
    )
    return call(
        join_kernel,
        shape((tok_rows, features), BF16),
        (stored, mine, across(theirs)),
        tok_rows * features,
        8,
    )


def solution(mesh):
    in_specs = (
        P("sp", "tp"),
        P("tp", None, None),
        P("tp"),
        P(None, "tp"),
        P("sp", "tp"),
        P("tp"),
        P("sp", None),
        P("sp", None),
        P("sp", None, "tp"),
        P("sp", None, "tp"),
        P("sp", "tp", None),
    )
    out_specs = P("sp", "tp")

    return jax.shard_map(on_device, mesh=mesh, in_specs=in_specs, out_specs=out_specs, check_vma=False)
```

```python
import functools

import jax
import jax.numpy as jnp
from jax import lax
from jax.experimental import pallas as pl
from jax.experimental.pallas import tpu as pltpu
from jax.sharding import PartitionSpec as P


GSIZE = 64
TOPK = 2
CORES = 2

GATE_LIMIT = 7.0
GATE_ALPHA = 1.702
NORM_EPS = 1e-05

F32 = jnp.float32
BF16 = jnp.bfloat16
MIB = 1024 * 1024


def iota(shape, dim):
    return lax.broadcasted_iota(jnp.int32, shape, dim)


def mm(a, b, ca=1, cb=0):
    return lax.dot_general(a, b, (((ca,), (cb,)), ((), ())), preferred_element_type=F32)


def call(kernel, out_shape, args, flops, mib, aliases=None, space=pltpu.VMEM, scratch=()):
    return pl.pallas_call(
        kernel,
        out_shape=out_shape,
        in_specs=[pl.BlockSpec(memory_space=space)] * len(args),
        scratch_shapes=scratch,
        out_specs=jax.tree.map(lambda _: pl.BlockSpec(memory_space=pltpu.VMEM), out_shape),
        compiler_params=pltpu.CompilerParams(vmem_limit_bytes=mib * MIB),
        cost_estimate=pl.CostEstimate(flops=flops, bytes_accessed=flops // 512, transcendentals=0),
        input_output_aliases=aliases or {},
    )(*args)


def pool_kernel(before_ref, x_ref, w_ref, gain_ref, norm_ref, out_ref):
    width, rows = x_ref.shape
    window = lax.shift_left(jnp.int32(2), lax.rem(lax.axis_index("tp"), 4))
    place = iota((rows, rows), 1) - iota((rows, rows), 0)
    inside = jnp.where((place >= 0) & (place < window), 1.0, 0.0).astype(BF16)
    reach = before_ref.shape[1]
    gap = iota((reach, rows), 1) + reach - iota((reach, rows), 0)
    behind = jnp.where(gap < window, 1.0, 0.0).astype(BF16)
    x = x_ref[...]
    total = mm(x, inside) + mm(before_ref[...], behind)
    spot = lax.axis_index("sp") * rows + iota((1, rows), 1)
    count = jnp.minimum(spot + 1, window).astype(F32)
    pooled = (total / count - x.astype(F32)).astype(BF16)
    eye = iota((width, width), 0) == iota((width, width), 1)
    gain = jnp.sum(jnp.where(eye, gain_ref[...].astype(F32), 0.0), axis=1, keepdims=True)
    out_ref[:width, :] = (mm(w_ref[...], pooled, 0, 0) * gain).astype(BF16)
    features = norm_ref.shape[1]
    tail = out_ref.shape[0] - width
    out_ref[width:, :features] = jnp.broadcast_to(norm_ref[...].astype(F32), (tail, features)).astype(BF16)
    out_ref[width:, features:] = jnp.zeros((tail, out_ref.shape[1] - features), BF16)


def row_slots(routes_ref, experts, capacity):
    rows = routes_ref.shape[1]
    named = [iota((experts, rows), 0) == routes_ref[k : k + 1, :] for k in range(TOPK)]
    ones = sum(jnp.where(n, 1.0, 0.0) for n in named)
    upper = jnp.where(iota((rows, rows), 0) < iota((rows, rows), 1), 1.0, 0.0).astype(BF16)
    earlier = mm(ones.astype(BF16), upper)
    slots = []
    for k in range(TOPK):
        rank = jnp.sum(jnp.where(named[k], earlier, 0.0), axis=0, keepdims=True).astype(jnp.int32)
        slots.append(routes_ref[k : k + 1, :] * capacity + rank)
    return slots


def slot_ids(shape, dim, capacity, core):
    half = capacity // CORES
    place = iota(shape, dim)
    return lax.div(place, half) * capacity + core * half + lax.rem(place, half)


class Pack:
    def __init__(self, deep, width, channels, rows):
        self.gate, self.up, self.down = 0, deep, 2 * deep
        self.project = 3 * deep
        self.resid = self.project + channels // 2
        self.rows = self.resid + rows // 2
        self.width = width


def prep_kernel(pack, gate, up, down, project, resid, x, w, gain, norm, out, x_out, w_out, gain_out, norm_out, sems):
    width, features = pack.width, project.shape[1]
    units = down.shape[0]
    pairs = [(x, x_out), (w, w_out), (gain, gain_out), (norm, norm_out)]
    for base, source in ((pack.project, project), (pack.resid, resid)):
        half = source.shape[0] // 2
        for i in range(2):
            pairs.append(
                (source.at[i * half : (i + 1) * half, :],
                 out.at[base : base + half, i * features : (i + 1) * features])
            )
    pairs.append((gate, out.at[pack.gate : pack.up, :]))
    pairs.append((up, out.at[pack.up : pack.down, :]))
    for i in range(down.shape[1] // width):
        pairs.append(
            (down.at[:, i * width : (i + 1) * width], out.at[pack.down + i * units : pack.down + (i + 1) * units, :])
        )
    copies = [pltpu.make_async_copy(a, b, sems.at[i]) for i, (a, b) in enumerate(pairs)]
    for copy in copies:
        copy.start()
    for copy in copies:
        copy.wait()


def dispatch_kernel(pack, experts, capacity, mixed_ref, own_ref, other_ref, routes_ref, stream_ref, gain_ref, out_ref):
    core = lax.rem(lax.axis_index("tp"), CORES)
    members, _, rows = mixed_ref.shape
    features = stream_ref.shape[1]
    mixed = mixed_ref[:, :GSIZE, :].reshape(members * GSIZE, rows)
    deep = members * GSIZE // 2
    streams = []
    for ref in (own_ref, other_ref):
        halves = [ref[pack.project : pack.resid, i * features : (i + 1) * features] for i in range(2)]
        projected = mm(mixed[:deep], halves[0], 0, 0) + mm(mixed[deep:], halves[1], 0, 0)
        resid = jnp.concatenate(
            [ref[pack.resid : pack.rows, i * features : (i + 1) * features] for i in range(2)], axis=0
        )
        streams.append((resid.astype(F32) + projected).astype(BF16))
    own, other = streams
    stream_ref[...] = own
    for t in range(members):
        y, c = divmod(t, CORES)
        gain_ref[y, :, c * features : (c + 1) * features] = mixed_ref[t, GSIZE : GSIZE + 8, :features].astype(F32)
    slots = row_slots(routes_ref, experts, capacity)
    ids = slot_ids((out_ref.shape[0], rows), 0, capacity, core)
    hit = (slots[0] == ids) | (slots[1] == ids)
    chosen = jnp.where(hit, 1.0, 0.0).astype(BF16)
    out_ref[:, :features] = mm(chosen, jnp.where(core == 0, own, other)).astype(BF16)
    out_ref[:, features:] = mm(chosen, jnp.where(core == 0, other, own)).astype(BF16)


def add_chunk(pack, x, chip, gain_ref, packs, acc_ref, square_ref, first=False):
    width = x.shape[1]
    value = x.astype(F32)
    square = value * value
    lanes = square_ref.shape[1]
    square = sum(square[:, i : i + lanes] for i in range(0, width, lanes))
    scaled = (value * gain_ref[chip, 0:1, :]).astype(BF16)
    for i, base in enumerate((pack.gate, pack.up)):
        for j, ref in enumerate(packs):
            rows = pl.ds(pl.multiple_of(base + chip * width, width), width)
            part = mm(scaled, ref[rows, :])
            columns = part.shape[1]
            span = slice((2 * i + j) * columns, (2 * i + j + 1) * columns)
            acc_ref[:, span] = part if first else acc_ref[:, span] + part
    square_ref[...] = square if first else square_ref[...] + square


def chip_at(chips, step):
    here, core = lax.div(lax.axis_index("tp"), CORES), lax.rem(lax.axis_index("tp"), CORES)
    return lax.rem(here + step * (1 - 2 * core) + chips, chips)


def first_kernel(pack, chips, x_ref, gain_ref, own_ref, other_ref, acc_ref, square_ref):
    add_chunk(pack, x_ref[...], chip_at(chips, 0), gain_ref, (own_ref, other_ref), acc_ref, square_ref, True)


def both_kernel(pack, chips, step, p_ref, m_ref, gain_ref, own_ref, other_ref, acc_in, square_in, acc_ref, square_ref):
    packs = (own_ref, other_ref)
    add_chunk(pack, p_ref[...], chip_at(chips, -step), gain_ref, packs, acc_ref, square_ref)
    add_chunk(pack, m_ref[...], chip_at(chips, step), gain_ref, packs, acc_ref, square_ref)


def partial(pack, hidden_ref, packs, chip):
    units = hidden_ref.shape[1] // CORES
    rows = pl.ds(pl.multiple_of(pack.down + chip * units, units), units)
    return sum(mm(hidden_ref[:, i * units : (i + 1) * units], ref[rows, :]) for i, ref in enumerate(packs))


def last_kernel(
    pack, chips, total, p_ref, gain_ref, own_ref, other_ref, acc_in, square_in, acc_ref, square_ref, hidden_ref, up_ref, low_ref
):
    packs = (own_ref, other_ref)
    far = chip_at(chips, chips // 2)
    add_chunk(pack, p_ref[...], far, gain_ref, packs, acc_ref, square_ref)
    mean = jnp.sum(square_ref[...], axis=1, keepdims=True) / total
    scale = lax.rsqrt(mean + NORM_EPS)
    units = hidden_ref.shape[1]
    gate = jnp.minimum(acc_ref[:, :units] * scale, GATE_LIMIT)
    up = jnp.clip(acc_ref[:, units:] * scale, -GATE_LIMIT, GATE_LIMIT)
    hidden_ref[...] = ((up + 1.0) * gate * jax.nn.sigmoid(GATE_ALPHA * gate)).astype(BF16)
    up_ref[...] = partial(pack, hidden_ref, packs, far).astype(BF16)
    low_ref[...] = partial(pack, hidden_ref, packs, chip_at(chips, 1 - chips // 2)).astype(BF16)


def down_kernel(pack, chips, steps, hidden_ref, own_ref, other_ref, *outs):
    for step, out_ref in zip(steps, outs):
        out_ref[...] = partial(pack, hidden_ref, (own_ref, other_ref), chip_at(chips, step))


def add_kernel(part_ref, came_ref, out_ref):
    out_ref[...] = (part_ref[...] + came_ref[...].astype(F32)).astype(BF16)


def own_kernel(part_ref, p_ref, m_ref, out_ref):
    out_ref[...] = (part_ref[...] + p_ref[...].astype(F32) + m_ref[...].astype(F32)).astype(BF16)


def pick_kernel(experts, capacity, back_ref, routes_ref, weight_ref, mine_ref, other_ref):
    core = lax.rem(lax.axis_index("tp"), CORES)
    slots = row_slots(routes_ref, experts, capacity)
    tokens = routes_ref.shape[1]
    ids = slot_ids((back_ref.shape[0], tokens), 0, capacity, core)
    eye = iota((tokens, tokens), 0) == iota((tokens, tokens), 1)
    rows = back_ref[...]
    total = 0.0
    for k in range(TOPK):
        chosen = jnp.where(slots[k] == ids, 1.0, 0.0).astype(BF16)
        weight = jnp.sum(jnp.where(eye, weight_ref[k : k + 1, :], 0.0), axis=1, keepdims=True)
        total = total + mm(chosen, rows, 0, 0) * weight
    features = mine_ref.shape[1]
    left, right = total[:, :features], total[:, features:]
    mine_ref[...] = jnp.where(core == 0, left, right)
    other_ref[...] = jnp.where(core == 0, right, left)


def join_kernel(stream_ref, mine_ref, other_ref, out_ref):
    out_ref[...] = (stream_ref[...].astype(F32) + mine_ref[...] + other_ref[...]).astype(BF16)


def on_device(
    pool_input,
    pool_weight,
    pool_gain,
    out_weight,
    resid,
    norm_gain,
    routes,
    route_weight,
    expert_gate,
    expert_up,
    expert_down,
):
    tok_rows, channels = pool_input.shape
    features = out_weight.shape[1]
    blocks, members = lax.axis_size("sp"), lax.axis_size("tp")
    chips = members // CORES
    experts = blocks * expert_gate.shape[0]
    capacity = 2 * tok_rows * TOPK // experts
    half = capacity // CORES
    width = features * CORES
    total = features * members
    held = blocks * half

    def along(value, step):
        pairs = [
            (y * CORES + c, (y + step * (1 - 2 * c)) % chips * CORES + c) for y in range(chips) for c in range(CORES)
        ]
        return lax.ppermute(value, "tp", pairs)

    def across(value):
        return lax.ppermute(value, "tp", [(t, t ^ 1) for t in range(members)])

    shape = jax.ShapeDtypeStruct
    deep, units = expert_gate.shape[1:]
    pack = Pack(deep, width, out_weight.shape[0], tok_rows)
    before = lax.ppermute(
        pool_input.T, "sp", [(s, s + 1) for s in range(blocks - 1)]
    )
    small = (pool_input.T, pool_weight[0], pool_gain.reshape(1, channels), norm_gain.reshape(1, features))
    own, *small = call(
        functools.partial(prep_kernel, pack),
        (pltpu.VMEM((pack.rows, width), BF16), *(pltpu.VMEM(v.shape, v.dtype) for v in small)),
        tuple(
            pltpu.with_memory_space_constraint(v, pltpu.HBM)
            for v in (expert_gate[0], expert_up[0], expert_down[0], out_weight, resid, *small)
        ),
        pack.rows * width * 512,
        8,
        space=pltpu.HBM,
        scratch=[pltpu.SemaphoreType.DMA((10 + chips,))],
    )
    other = across(own)
    packs = (own, other)
    pooled = call(
        pool_kernel,
        shape((GSIZE + 16, tok_rows), BF16),
        (before, *small),
        tok_rows * tok_rows * channels * 2,
        8,
    )
    mixed = lax.all_gather(pooled, "tp", axis=0, tiled=False)
    stored, gains, sent = call(
        functools.partial(dispatch_kernel, pack, experts, capacity),
        (
            shape((tok_rows, features), BF16),
            shape((chips, 8, width), F32),
            shape((experts * half, width), BF16),
        ),
        (mixed, *packs, routes.T),
        2 * experts * half * width * tok_rows,
        16,
    )
    x = lax.all_to_all(
        sent.reshape(experts, half, width), "sp", split_axis=0, concat_axis=0, tiled=True
    ).reshape(held, width)

    acc_shape = (shape((held, 4 * units), F32), shape((held, 128), F32))
    chunk_flops = 2 * held * width * 4 * units
    acc, square = call(
        functools.partial(first_kernel, pack, chips), acc_shape, (x, gains, *packs), chunk_flops, 16
    )
    ahead, back = x, x
    last = chips // 2
    for step in range(1, last):
        ahead = along(ahead, 1)
        back = along(back, -1)
        acc, square = call(
            functools.partial(both_kernel, pack, chips, step),
            acc_shape,
            (ahead, back, gains, *packs, acc, square),
            2 * chunk_flops,
            16,
            {5: 0, 6: 1},
        )
    ahead = along(ahead, 1)
    _, _, hidden, ahead, back = call(
        functools.partial(last_kernel, pack, chips, float(total)),
        (*acc_shape, shape((held, CORES * units), BF16), *(shape((held, width), BF16),) * 2),
        (ahead, gains, *packs, acc, square),
        2 * chunk_flops,
        24,
        {4: 0, 5: 1},
    )

    def joined(part, came):
        return call(add_kernel, shape((held, width), BF16), (part, came), held * width, 8)

    steps = [*range(last - 1, -1, -1), *range(2 - last, 0)]
    parts = call(
        functools.partial(down_kernel, pack, chips, steps),
        (shape((held, width), F32),) * len(steps),
        (hidden, *packs),
        chunk_flops // 2 * len(steps),
        24,
    )
    part = dict(zip(steps, parts))
    for step in range(last - 1, -1, -1):
        ahead = along(ahead, 1)
        if step:
            back = along(back, -1)
            ahead = joined(part[step], ahead)
            back = joined(part[1 - step], back) if step > 1 else back
    result = call(own_kernel, pltpu.VMEM((held, width), BF16), (part[0], ahead, back), held * width, 8)
    returned = lax.all_to_all(
        result.reshape(blocks, half, width), "sp", split_axis=0, concat_axis=0, tiled=True
    ).reshape(experts * half, width)
    mine, theirs = call(
        functools.partial(pick_kernel, experts, capacity),
        (shape((tok_rows, features), F32),) * 2,
        (returned, routes.T, route_weight.T),
        4 * experts * half * width * tok_rows,
        12,
    )
    return call(
        join_kernel,
        shape((tok_rows, features), BF16),
        (stored, mine, across(theirs)),
        tok_rows * features,
        8,
    )


def solution(mesh):
    in_specs = (
        P("sp", "tp"),
        P("tp", None, None),
        P("tp"),
        P(None, "tp"),
        P("sp", "tp"),
        P("tp"),
        P("sp", None),
        P("sp", None),
        P("sp", None, "tp"),
        P("sp", None, "tp"),
        P("sp", "tp", None),
    )
    out_specs = P("sp", "tp")

    return jax.shard_map(on_device, mesh=mesh, in_specs=in_specs, out_specs=out_specs, check_vma=False)
```

```python
import functools

import jax
import jax.numpy as jnp
from jax import lax
from jax.experimental import pallas as pl
from jax.experimental.pallas import tpu as pltpu
from jax.sharding import PartitionSpec as P


GSIZE = 64
TOPK = 2
CORES = 2

GATE_LIMIT = 7.0
GATE_ALPHA = 1.702
NORM_EPS = 1e-05

F32 = jnp.float32
BF16 = jnp.bfloat16
MIB = 1024 * 1024


def iota(shape, dim):
    return lax.broadcasted_iota(jnp.int32, shape, dim)


def mm(a, b, ca=1, cb=0):
    return lax.dot_general(a, b, (((ca,), (cb,)), ((), ())), preferred_element_type=F32)


def call(kernel, out_shape, args, flops, mib, aliases=None, space=pltpu.VMEM, scratch=()):
    return pl.pallas_call(
        kernel,
        out_shape=out_shape,
        in_specs=[pl.BlockSpec(memory_space=space)] * len(args),
        scratch_shapes=scratch,
        out_specs=jax.tree.map(lambda _: pl.BlockSpec(memory_space=pltpu.VMEM), out_shape),
        compiler_params=pltpu.CompilerParams(vmem_limit_bytes=mib * MIB),
        cost_estimate=pl.CostEstimate(flops=flops, bytes_accessed=flops // 512, transcendentals=0),
        input_output_aliases=aliases or {},
    )(*args)


def pool_kernel(before_ref, x_ref, w_ref, gain_ref, norm_ref, out_ref):
    width, rows = x_ref.shape
    window = lax.shift_left(jnp.int32(2), lax.rem(lax.axis_index("tp"), 4))
    place = iota((rows, rows), 1) - iota((rows, rows), 0)
    inside = jnp.where((place >= 0) & (place < window), 1.0, 0.0).astype(BF16)
    reach = before_ref.shape[1]
    gap = iota((reach, rows), 1) + reach - iota((reach, rows), 0)
    behind = jnp.where(gap < window, 1.0, 0.0).astype(BF16)
    x = x_ref[...]
    total = mm(x, inside) + mm(before_ref[...], behind)
    spot = lax.axis_index("sp") * rows + iota((1, rows), 1)
    count = jnp.minimum(spot + 1, window).astype(F32)
    pooled = (total / count - x.astype(F32)).astype(BF16)
    eye = iota((width, width), 0) == iota((width, width), 1)
    gain = jnp.sum(jnp.where(eye, gain_ref[...].astype(F32), 0.0), axis=1, keepdims=True)
    out_ref[:width, :] = (mm(w_ref[...], pooled, 0, 0) * gain).astype(BF16)
    features = norm_ref.shape[1]
    tail = out_ref.shape[0] - width
    out_ref[width:, :features] = jnp.broadcast_to(norm_ref[...].astype(F32), (tail, features)).astype(BF16)
    out_ref[width:, features:] = jnp.zeros((tail, out_ref.shape[1] - features), BF16)


def row_slots(routes_ref, experts, capacity):
    rows = routes_ref.shape[1]
    named = [iota((experts, rows), 0) == routes_ref[k : k + 1, :] for k in range(TOPK)]
    ones = sum(jnp.where(n, 1.0, 0.0) for n in named)
    upper = jnp.where(iota((rows, rows), 0) < iota((rows, rows), 1), 1.0, 0.0).astype(BF16)
    earlier = mm(ones.astype(BF16), upper)
    slots = []
    for k in range(TOPK):
        rank = jnp.sum(jnp.where(named[k], earlier, 0.0), axis=0, keepdims=True).astype(jnp.int32)
        slots.append(routes_ref[k : k + 1, :] * capacity + rank)
    return slots


def slot_ids(shape, dim, capacity, core):
    half = capacity // CORES
    place = iota(shape, dim)
    return lax.div(place, half) * capacity + core * half + lax.rem(place, half)


class Pack:
    def __init__(self, deep, width, channels, rows):
        self.gate, self.up, self.down = 0, deep, 2 * deep
        self.project = 3 * deep
        self.resid = self.project + channels // 2
        self.rows = self.resid + rows // 2
        self.width = width


def prep_kernel(pack, gate, up, down, project, resid, x, w, gain, norm, out, x_out, w_out, gain_out, norm_out, sems):
    width, features = pack.width, project.shape[1]
    units = down.shape[0]
    pairs = [(x, x_out), (w, w_out), (gain, gain_out), (norm, norm_out)]
    for base, source in ((pack.project, project), (pack.resid, resid)):
        half = source.shape[0] // 2
        for i in range(2):
            pairs.append(
                (source.at[i * half : (i + 1) * half, :],
                 out.at[base : base + half, i * features : (i + 1) * features])
            )
    pairs.append((gate, out.at[pack.gate : pack.up, :]))
    pairs.append((up, out.at[pack.up : pack.down, :]))
    for i in range(down.shape[1] // width):
        pairs.append(
            (down.at[:, i * width : (i + 1) * width], out.at[pack.down + i * units : pack.down + (i + 1) * units, :])
        )
    copies = [pltpu.make_async_copy(a, b, sems.at[i]) for i, (a, b) in enumerate(pairs)]
    for copy in copies:
        copy.start()
    for copy in copies:
        copy.wait()


def dispatch_kernel(pack, experts, capacity, mixed_ref, own_ref, other_ref, routes_ref, stream_ref, gain_ref, out_ref):
    core = lax.rem(lax.axis_index("tp"), CORES)
    members, _, rows = mixed_ref.shape
    features = stream_ref.shape[1]
    mixed = mixed_ref[:, :GSIZE, :].reshape(members * GSIZE, rows)
    deep = members * GSIZE // 2
    streams = []
    for ref in (own_ref, other_ref):
        halves = [ref[pack.project : pack.resid, i * features : (i + 1) * features] for i in range(2)]
        projected = mm(mixed[:deep], halves[0], 0, 0) + mm(mixed[deep:], halves[1], 0, 0)
        resid = jnp.concatenate(
            [ref[pack.resid : pack.rows, i * features : (i + 1) * features] for i in range(2)], axis=0
        )
        streams.append((resid.astype(F32) + projected).astype(BF16))
    own, other = streams
    stream_ref[...] = own
    for t in range(members):
        y, c = divmod(t, CORES)
        gain_ref[y, :, c * features : (c + 1) * features] = mixed_ref[t, GSIZE : GSIZE + 8, :features].astype(F32)
    slots = row_slots(routes_ref, experts, capacity)
    ids = slot_ids((out_ref.shape[0], rows), 0, capacity, core)
    hit = (slots[0] == ids) | (slots[1] == ids)
    chosen = jnp.where(hit, 1.0, 0.0).astype(BF16)
    out_ref[:, :features] = mm(chosen, jnp.where(core == 0, own, other)).astype(BF16)
    out_ref[:, features:] = mm(chosen, jnp.where(core == 0, other, own)).astype(BF16)


def add_chunk(pack, x, chip, gain_ref, packs, acc_ref, square_ref, first=False):
    width = x.shape[1]
    value = x.astype(F32)
    square = value * value
    lanes = square_ref.shape[1]
    square = sum(square[:, i : i + lanes] for i in range(0, width, lanes))
    scaled = (value * gain_ref[chip, 0:1, :]).astype(BF16)
    for i, base in enumerate((pack.gate, pack.up)):
        for j, ref in enumerate(packs):
            rows = pl.ds(pl.multiple_of(base + chip * width, width), width)
            part = mm(scaled, ref[rows, :])
            columns = part.shape[1]
            span = slice((2 * i + j) * columns, (2 * i + j + 1) * columns)
            acc_ref[:, span] = part if first else acc_ref[:, span] + part
    square_ref[...] = square if first else square_ref[...] + square


def chip_at(chips, step):
    here = lax.div(lax.axis_index("tp"), CORES)
    return lax.rem(here + step + chips, chips)


def chip_across(chips, step):
    core = lax.rem(lax.axis_index("tp"), CORES)
    return chip_at(chips, step * (1 - 2 * core))


def first_kernel(pack, chips, x_ref, gain_ref, own_ref, other_ref, acc_ref, square_ref):
    add_chunk(pack, x_ref[...], chip_at(chips, 0), gain_ref, (own_ref, other_ref), acc_ref, square_ref, True)


def both_kernel(pack, chips, step, p_ref, m_ref, gain_ref, own_ref, other_ref, acc_in, square_in, acc_ref, square_ref):
    packs = (own_ref, other_ref)
    add_chunk(pack, p_ref[...], chip_at(chips, -step), gain_ref, packs, acc_ref, square_ref)
    add_chunk(pack, m_ref[...], chip_at(chips, step), gain_ref, packs, acc_ref, square_ref)


def partial(pack, hidden_ref, packs, chip):
    units = hidden_ref.shape[1] // CORES
    rows = pl.ds(pl.multiple_of(pack.down + chip * units, units), units)
    return sum(mm(hidden_ref[:, i * units : (i + 1) * units], ref[rows, :]) for i, ref in enumerate(packs))


def last_kernel(
    pack, chips, total, p_ref, gain_ref, own_ref, other_ref, acc_in, square_in, acc_ref, square_ref, hidden_ref, up_ref, low_ref
):
    packs = (own_ref, other_ref)
    far = chip_at(chips, chips // 2)
    add_chunk(pack, p_ref[...], far, gain_ref, packs, acc_ref, square_ref)
    mean = jnp.sum(square_ref[...], axis=1, keepdims=True) / total
    scale = lax.rsqrt(mean + NORM_EPS)
    units = hidden_ref.shape[1]
    gate = jnp.minimum(acc_ref[:, :units] * scale, GATE_LIMIT)
    up = jnp.clip(acc_ref[:, units:] * scale, -GATE_LIMIT, GATE_LIMIT)
    hidden_ref[...] = ((up + 1.0) * gate * jax.nn.sigmoid(GATE_ALPHA * gate)).astype(BF16)
    up_ref[...] = partial(pack, hidden_ref, packs, far).astype(BF16)
    low_ref[...] = partial(pack, hidden_ref, packs, chip_across(chips, 1 - chips // 2)).astype(BF16)


def down_kernel(pack, chips, steps, hidden_ref, own_ref, other_ref, *outs):
    for step, out_ref in zip(steps, outs):
        out_ref[...] = partial(pack, hidden_ref, (own_ref, other_ref), chip_across(chips, step))


def add_kernel(part_ref, came_ref, out_ref):
    out_ref[...] = (part_ref[...] + came_ref[...].astype(F32)).astype(BF16)


def own_kernel(part_ref, p_ref, m_ref, out_ref):
    out_ref[...] = (part_ref[...] + p_ref[...].astype(F32) + m_ref[...].astype(F32)).astype(BF16)


def pick_kernel(experts, capacity, back_ref, routes_ref, weight_ref, mine_ref, other_ref):
    core = lax.rem(lax.axis_index("tp"), CORES)
    slots = row_slots(routes_ref, experts, capacity)
    tokens = routes_ref.shape[1]
    ids = slot_ids((back_ref.shape[0], tokens), 0, capacity, core)
    eye = iota((tokens, tokens), 0) == iota((tokens, tokens), 1)
    rows = back_ref[...]
    total = 0.0
    for k in range(TOPK):
        chosen = jnp.where(slots[k] == ids, 1.0, 0.0).astype(BF16)
        weight = jnp.sum(jnp.where(eye, weight_ref[k : k + 1, :], 0.0), axis=1, keepdims=True)
        total = total + mm(chosen, rows, 0, 0) * weight
    features = mine_ref.shape[1]
    left, right = total[:, :features], total[:, features:]
    mine_ref[...] = jnp.where(core == 0, left, right)
    other_ref[...] = jnp.where(core == 0, right, left)


def join_kernel(stream_ref, mine_ref, other_ref, out_ref):
    out_ref[...] = (stream_ref[...].astype(F32) + mine_ref[...] + other_ref[...]).astype(BF16)


def on_device(
    pool_input,
    pool_weight,
    pool_gain,
    out_weight,
    resid,
    norm_gain,
    routes,
    route_weight,
    expert_gate,
    expert_up,
    expert_down,
):
    tok_rows, channels = pool_input.shape
    features = out_weight.shape[1]
    blocks, members = lax.axis_size("sp"), lax.axis_size("tp")
    chips = members // CORES
    experts = blocks * expert_gate.shape[0]
    capacity = 2 * tok_rows * TOPK // experts
    half = capacity // CORES
    width = features * CORES
    total = features * members
    held = blocks * half

    def along(value, step, other=1):
        pairs = [(y * CORES, (y + step) % chips * CORES) for y in range(chips)]
        pairs += [(y * CORES + 1, (y + step * other) % chips * CORES + 1) for y in range(chips)]
        return lax.ppermute(value, "tp", pairs)

    def across(value):
        return lax.ppermute(value, "tp", [(t, t ^ 1) for t in range(members)])

    shape = jax.ShapeDtypeStruct
    deep, units = expert_gate.shape[1:]
    pack = Pack(deep, width, out_weight.shape[0], tok_rows)
    before = lax.ppermute(
        pool_input.T, "sp", [(s, s + 1) for s in range(blocks - 1)]
    )
    small = (pool_input.T, pool_weight[0], pool_gain.reshape(1, channels), norm_gain.reshape(1, features))
    own, *small = call(
        functools.partial(prep_kernel, pack),
        (pltpu.VMEM((pack.rows, width), BF16), *(pltpu.VMEM(v.shape, v.dtype) for v in small)),
        tuple(
            pltpu.with_memory_space_constraint(v, pltpu.HBM)
            for v in (expert_gate[0], expert_up[0], expert_down[0], out_weight, resid, *small)
        ),
        pack.rows * width * 512,
        8,
        space=pltpu.HBM,
        scratch=[pltpu.SemaphoreType.DMA((10 + chips,))],
    )
    other = across(own)
    packs = (own, other)
    pooled = call(
        pool_kernel,
        shape((GSIZE + 16, tok_rows), BF16),
        (before, *small),
        tok_rows * tok_rows * channels * 2,
        8,
    )
    mixed = lax.all_gather(pooled, "tp", axis=0, tiled=False)
    stored, gains, sent = call(
        functools.partial(dispatch_kernel, pack, experts, capacity),
        (
            shape((tok_rows, features), BF16),
            shape((chips, 8, width), F32),
            shape((experts * half, width), BF16),
        ),
        (mixed, *packs, routes.T),
        2 * experts * half * width * tok_rows,
        16,
    )
    x = lax.all_to_all(
        sent.reshape(experts, half, width), "sp", split_axis=0, concat_axis=0, tiled=True
    ).reshape(held, width)

    acc_shape = (shape((held, 4 * units), F32), shape((held, 128), F32))
    chunk_flops = 2 * held * width * 4 * units
    acc, square = call(
        functools.partial(first_kernel, pack, chips), acc_shape, (x, gains, *packs), chunk_flops, 16
    )
    ahead, back = x, x
    last = chips // 2
    for step in range(1, last):
        ahead = along(ahead, 1)
        back = along(back, -1)
        acc, square = call(
            functools.partial(both_kernel, pack, chips, step),
            acc_shape,
            (ahead, back, gains, *packs, acc, square),
            2 * chunk_flops,
            16,
            {5: 0, 6: 1},
        )
    ahead = along(ahead, 1)
    _, _, hidden, ahead, back = call(
        functools.partial(last_kernel, pack, chips, float(total)),
        (*acc_shape, shape((held, CORES * units), BF16), *(shape((held, width), BF16),) * 2),
        (ahead, gains, *packs, acc, square),
        2 * chunk_flops,
        24,
        {4: 0, 5: 1},
    )

    def joined(part, came):
        return call(add_kernel, shape((held, width), BF16), (part, came), held * width, 8)

    steps = [*range(last - 1, -1, -1), *range(2 - last, 0)]
    parts = call(
        functools.partial(down_kernel, pack, chips, steps),
        (shape((held, width), F32),) * len(steps),
        (hidden, *packs),
        chunk_flops // 2 * len(steps),
        24,
    )
    part = dict(zip(steps, parts))
    for step in range(last - 1, -1, -1):
        ahead = along(ahead, 1, -1)
        if step:
            back = along(back, -1, -1)
            ahead = joined(part[step], ahead)
            back = joined(part[1 - step], back) if step > 1 else back
    result = call(own_kernel, pltpu.VMEM((held, width), BF16), (part[0], ahead, back), held * width, 8)
    returned = lax.all_to_all(
        result.reshape(blocks, half, width), "sp", split_axis=0, concat_axis=0, tiled=True
    ).reshape(experts * half, width)
    mine, theirs = call(
        functools.partial(pick_kernel, experts, capacity),
        (shape((tok_rows, features), F32),) * 2,
        (returned, routes.T, route_weight.T),
        4 * experts * half * width * tok_rows,
        12,
    )
    return call(
        join_kernel,
        shape((tok_rows, features), BF16),
        (stored, mine, across(theirs)),
        tok_rows * features,
        8,
    )


def solution(mesh):
    in_specs = (
        P("sp", "tp"),
        P("tp", None, None),
        P("tp"),
        P(None, "tp"),
        P("sp", "tp"),
        P("tp"),
        P("sp", None),
        P("sp", None),
        P("sp", None, "tp"),
        P("sp", None, "tp"),
        P("sp", "tp", None),
    )
    out_specs = P("sp", "tp")

    return jax.shard_map(on_device, mesh=mesh, in_specs=in_specs, out_specs=out_specs, check_vma=False)
```

```python
import functools

import jax
import jax.numpy as jnp
from jax import lax
from jax.experimental import pallas as pl
from jax.experimental.pallas import tpu as pltpu
from jax.sharding import PartitionSpec as P


GSIZE = 64
TOPK = 2
CORES = 2

GATE_LIMIT = 7.0
GATE_ALPHA = 1.702
NORM_EPS = 1e-05

F32 = jnp.float32
BF16 = jnp.bfloat16
MIB = 1024 * 1024


def iota(shape, dim):
    return lax.broadcasted_iota(jnp.int32, shape, dim)


def mm(a, b, ca=1, cb=0):
    return lax.dot_general(a, b, (((ca,), (cb,)), ((), ())), preferred_element_type=F32)


def call(kernel, out_shape, args, flops, mib, aliases=None, space=pltpu.VMEM, scratch=()):
    return pl.pallas_call(
        kernel,
        out_shape=out_shape,
        in_specs=[pl.BlockSpec(memory_space=s) for s in (space if isinstance(space, tuple) else (space,) * len(args))],
        scratch_shapes=scratch,
        out_specs=jax.tree.map(lambda _: pl.BlockSpec(memory_space=pltpu.VMEM), out_shape),
        compiler_params=pltpu.CompilerParams(vmem_limit_bytes=mib * MIB),
        cost_estimate=pl.CostEstimate(flops=flops, bytes_accessed=flops // 512, transcendentals=0),
        input_output_aliases=aliases or {},
    )(*args)


def pool_kernel(before_ref, x_ref, w_ref, gain_ref, norm_ref, out_ref):
    width, rows = x_ref.shape
    window = lax.shift_left(jnp.int32(2), lax.rem(lax.axis_index("tp"), 4))
    place = iota((rows, rows), 1) - iota((rows, rows), 0)
    inside = jnp.where((place >= 0) & (place < window), 1.0, 0.0).astype(BF16)
    reach = before_ref.shape[1]
    gap = iota((reach, rows), 1) + reach - iota((reach, rows), 0)
    behind = jnp.where(gap < window, 1.0, 0.0).astype(BF16)
    x = x_ref[...]
    total = mm(x, inside) + mm(before_ref[...], behind)
    spot = lax.axis_index("sp") * rows + iota((1, rows), 1)
    count = jnp.minimum(spot + 1, window).astype(F32)
    pooled = (total / count - x.astype(F32)).astype(BF16)
    eye = iota((width, width), 0) == iota((width, width), 1)
    gain = jnp.sum(jnp.where(eye, gain_ref[...].astype(F32), 0.0), axis=1, keepdims=True)
    mixed = (mm(w_ref[...], pooled, 0, 0) * gain).astype(BF16)
    features = norm_ref.shape[1]
    tail = out_ref.shape[1] - width
    norm = jnp.broadcast_to(norm_ref[...].astype(F32), (tail, features)).astype(BF16)
    for i in range(out_ref.shape[0]):
        out_ref[i, :width, :] = mixed
        out_ref[i, width:, :features] = norm
        out_ref[i, width:, features:] = jnp.zeros((tail, rows - features), BF16)


def row_slots(routes_ref, experts, capacity):
    rows = routes_ref.shape[1]
    named = [iota((experts, rows), 0) == routes_ref[k : k + 1, :] for k in range(TOPK)]
    ones = sum(jnp.where(n, 1.0, 0.0) for n in named)
    upper = jnp.where(iota((rows, rows), 0) < iota((rows, rows), 1), 1.0, 0.0).astype(BF16)
    earlier = mm(ones.astype(BF16), upper)
    slots = []
    for k in range(TOPK):
        rank = jnp.sum(jnp.where(named[k], earlier, 0.0), axis=0, keepdims=True).astype(jnp.int32)
        slots.append(routes_ref[k : k + 1, :] * capacity + rank)
    return slots


def slot_ids(shape, dim, capacity, core):
    half = capacity // CORES
    place = iota(shape, dim)
    return lax.div(place, half) * capacity + core * half + lax.rem(place, half)


class Pack:
    def __init__(self, deep, width, channels, rows):
        self.gate, self.up, self.down = 0, deep, 2 * deep
        self.project = 3 * deep
        self.resid = self.project + channels // 2
        self.rows = self.resid + rows // 2
        self.width = width


def copy_all(pairs, sems):
    copies = [pltpu.make_async_copy(a, b, sems.at[i]) for i, (a, b) in enumerate(pairs)]
    for copy in copies:
        copy.start()
    for copy in copies:
        copy.wait()


def fetch_kernel(source, out, sem):
    copy = pltpu.make_async_copy(source.at[: out.shape[0], :], out, sem)
    copy.start()
    copy.wait()


def load_kernel(count, *refs):
    copy_all(list(zip(refs[:count], refs[count : 2 * count])), refs[2 * count])


def prep_kernel(pack, gate, up, down, project, resid, out, sems):
    width, features = pack.width, project.shape[1]
    units = down.shape[0]
    pairs = []
    for t in range(project.shape[0] // GSIZE):
        base, c = pack.project + t // CORES * GSIZE, t % CORES
        pairs.append(
            (project.at[t * GSIZE : (t + 1) * GSIZE, :],
             out.at[base : base + GSIZE, c * features : (c + 1) * features])
        )
    half = resid.shape[0] // 2
    for i in range(2):
        pairs.append(
            (resid.at[i * half : (i + 1) * half, :],
             out.at[pack.resid : pack.rows, i * features : (i + 1) * features])
        )
    pairs.append((gate, out.at[pack.gate : pack.up, :]))
    pairs.append((up, out.at[pack.up : pack.down, :]))
    for i in range(down.shape[1] // width):
        pairs.append(
            (down.at[:, i * width : (i + 1) * width], out.at[pack.down + i * units : pack.down + (i + 1) * units, :])
        )
    copy_all(pairs, sems)


def dispatch_kernel(
    pack, experts, capacity, near_ref, far_ref, own_ref, other_ref, routes_ref, stream_ref, gain_ref, out_ref,
    fetched_ref, sem,
):
    fetch = pltpu.make_async_copy(other_ref.at[pack.project : pack.rows, :], fetched_ref, sem)
    fetch.start()
    core = lax.rem(lax.axis_index("tp"), CORES)
    chips, _, rows = near_ref.shape
    features = stream_ref.shape[1]

    def by_core(mine, others):
        return jnp.where(core == 0, mine, others), jnp.where(core == 0, others, mine)

    near = near_ref[:, :GSIZE, :].reshape(chips * GSIZE, rows)
    far = far_ref[:, :GSIZE, :].reshape(chips * GSIZE, rows)

    def stream_of(ref, base):
        deep, end = base + pack.resid - pack.project, base + pack.rows - pack.project
        halves = [(ref[base:deep, lanes], ref[deep:end, lanes]) for lanes in (slice(0, features), slice(features, None))]
        mine, others = by_core(halves[0][0], halves[1][0])
        projected = mm(near, mine, 0, 0) + mm(far, others, 0, 0)
        resid = jnp.concatenate([halves[0][1], halves[1][1]], axis=0)
        return (resid.astype(F32) + projected).astype(BF16)

    own = stream_of(own_ref, pack.project)
    stream_ref[...] = own
    for y in range(chips):
        gains = (ref[y, GSIZE : GSIZE + 8, :features].astype(F32) for ref in (near_ref, far_ref))
        gain_ref[y, :, :features], gain_ref[y, :, features:] = by_core(*gains)
    slots = row_slots(routes_ref, experts, capacity)
    ids = slot_ids((out_ref.shape[0], rows), 0, capacity, core)
    hit = (slots[0] == ids) | (slots[1] == ids)
    chosen = jnp.where(hit, 1.0, 0.0).astype(BF16)
    fetch.wait()
    left, right = by_core(own, stream_of(fetched_ref, 0))
    out_ref[:, :features] = mm(chosen, left).astype(BF16)
    out_ref[:, features:] = mm(chosen, right).astype(BF16)


def add_chunk(pack, x, chip, gain_ref, packs, acc_ref, square_ref, first=False):
    width = x.shape[1]
    value = x.astype(F32)
    square = value * value
    lanes = square_ref.shape[1]
    square = sum(square[:, i : i + lanes] for i in range(0, width, lanes))
    scaled = (value * gain_ref[chip, 0:1, :]).astype(BF16)
    for i, base in enumerate((pack.gate, pack.up)):
        for j, ref in enumerate(packs):
            rows = pl.ds(pl.multiple_of(base + chip * width, width), width)
            part = mm(scaled, ref[rows, :])
            columns = part.shape[1]
            span = slice((2 * i + j) * columns, (2 * i + j + 1) * columns)
            acc_ref[:, span] = part if first else acc_ref[:, span] + part
    square_ref[...] = square if first else square_ref[...] + square


def chip_at(chips, step):
    here = lax.div(lax.axis_index("tp"), CORES)
    return lax.rem(here + step + chips, chips)


def chip_across(chips, step):
    core = lax.rem(lax.axis_index("tp"), CORES)
    return chip_at(chips, step * (1 - 2 * core))


def first_kernel(pack, chips, x_ref, gain_ref, own_ref, other_ref, acc_ref, square_ref):
    add_chunk(pack, x_ref[...], chip_at(chips, 0), gain_ref, (own_ref, other_ref), acc_ref, square_ref, True)


def both_kernel(pack, chips, step, p_ref, m_ref, gain_ref, own_ref, other_ref, acc_in, square_in, acc_ref, square_ref):
    packs = (own_ref, other_ref)
    add_chunk(pack, p_ref[...], chip_at(chips, -step), gain_ref, packs, acc_ref, square_ref)
    add_chunk(pack, m_ref[...], chip_at(chips, step), gain_ref, packs, acc_ref, square_ref)


def partial(pack, hidden_ref, packs, chip):
    units = hidden_ref.shape[1] // CORES
    rows = pl.ds(pl.multiple_of(pack.down + chip * units, units), units)
    return sum(mm(hidden_ref[:, i * units : (i + 1) * units], ref[rows, :]) for i, ref in enumerate(packs))


def last_kernel(
    pack, chips, total, p_ref, gain_ref, own_ref, other_ref, acc_in, square_in, acc_ref, square_ref, hidden_ref, up_ref, low_ref
):
    packs = (own_ref, other_ref)
    far = chip_at(chips, chips // 2)
    add_chunk(pack, p_ref[...], far, gain_ref, packs, acc_ref, square_ref)
    mean = jnp.sum(square_ref[...], axis=1, keepdims=True) / total
    scale = lax.rsqrt(mean + NORM_EPS)
    units = hidden_ref.shape[1]
    gate = jnp.minimum(acc_ref[:, :units] * scale, GATE_LIMIT)
    up = jnp.clip(acc_ref[:, units:] * scale, -GATE_LIMIT, GATE_LIMIT)
    hidden_ref[...] = ((up + 1.0) * gate * jax.nn.sigmoid(GATE_ALPHA * gate)).astype(BF16)
    up_ref[...] = partial(pack, hidden_ref, packs, far).astype(BF16)
    low_ref[...] = partial(pack, hidden_ref, packs, chip_across(chips, 1 - chips // 2)).astype(BF16)


def down_kernel(pack, chips, steps, hidden_ref, own_ref, other_ref, *outs):
    for step, out_ref in zip(steps, outs):
        out_ref[...] = partial(pack, hidden_ref, (own_ref, other_ref), chip_across(chips, step))


def add_kernel(part_ref, came_ref, out_ref):
    out_ref[...] = (part_ref[...] + came_ref[...].astype(F32)).astype(BF16)


def own_kernel(part_ref, p_ref, m_ref, out_ref):
    out_ref[...] = (part_ref[...] + p_ref[...].astype(F32) + m_ref[...].astype(F32)).astype(BF16)


def pick_kernel(experts, capacity, back_ref, routes_ref, weight_ref, mine_ref, other_ref):
    core = lax.rem(lax.axis_index("tp"), CORES)
    slots = row_slots(routes_ref, experts, capacity)
    tokens = routes_ref.shape[1]
    ids = slot_ids((back_ref.shape[0], tokens), 0, capacity, core)
    eye = iota((tokens, tokens), 0) == iota((tokens, tokens), 1)
    rows = back_ref[...]
    total = 0.0
    for k in range(TOPK):
        chosen = jnp.where(slots[k] == ids, 1.0, 0.0).astype(BF16)
        weight = jnp.sum(jnp.where(eye, weight_ref[k : k + 1, :], 0.0), axis=1, keepdims=True)
        total = total + mm(chosen, rows, 0, 0) * weight
    features = mine_ref.shape[1]
    left, right = total[:, :features], total[:, features:]
    mine_ref[...] = jnp.where(core == 0, left, right)
    other_ref[...] = jnp.where(core == 0, right, left)


def join_kernel(stream_ref, mine_ref, other_ref, out_ref):
    out_ref[...] = (stream_ref[...].astype(F32) + mine_ref[...] + other_ref[...]).astype(BF16)


def on_device(
    pool_input,
    pool_weight,
    pool_gain,
    out_weight,
    resid,
    norm_gain,
    routes,
    route_weight,
    expert_gate,
    expert_up,
    expert_down,
):
    tok_rows, channels = pool_input.shape
    features = out_weight.shape[1]
    blocks, members = lax.axis_size("sp"), lax.axis_size("tp")
    chips = members // CORES
    experts = blocks * expert_gate.shape[0]
    capacity = 2 * tok_rows * TOPK // experts
    half = capacity // CORES
    width = features * CORES
    total = features * members
    held = blocks * half

    def along(value, step, other=1):
        pairs = [(y * CORES, (y + step) % chips * CORES) for y in range(chips)]
        pairs += [(y * CORES + 1, (y + step * other) % chips * CORES + 1) for y in range(chips)]
        return lax.ppermute(value, "tp", pairs)

    def across(value):
        return lax.ppermute(value, "tp", [(t, t ^ 1) for t in range(members)])

    shape = jax.ShapeDtypeStruct
    deep, units = expert_gate.shape[1:]
    pack = Pack(deep, width, out_weight.shape[0], tok_rows)
    before = lax.ppermute(
        pool_input.T, "sp", [(s, s + 1) for s in range(blocks - 1)]
    )

    def in_hbm(*values):
        return tuple(pltpu.with_memory_space_constraint(v, pltpu.HBM) for v in values)

    small = (pool_input.T, pool_weight[0], pool_gain.reshape(1, channels), norm_gain.reshape(1, features))
    small = call(
        functools.partial(load_kernel, len(small)),
        tuple(pltpu.VMEM(v.shape, v.dtype) for v in small),
        in_hbm(*small),
        tok_rows * 512,
        8,
        space=pl.ANY,
        scratch=[pltpu.SemaphoreType.DMA((len(small),))],
    )
    pooled = call(
        pool_kernel,
        shape((chips, GSIZE + 16, tok_rows), BF16),
        (before, *small),
        tok_rows * tok_rows * channels * 2,
        8,
    )
    near = lax.all_to_all(
        pooled, "tp", split_axis=0, concat_axis=0, tiled=True,
        axis_index_groups=[[y * CORES + c for y in range(chips)] for c in range(CORES)],
    )
    (own,) = call(
        functools.partial(prep_kernel, pack),
        (pltpu.VMEM((pack.rows, width), BF16),),
        in_hbm(expert_gate[0], expert_up[0], expert_down[0], out_weight, resid),
        pack.rows * width * 512,
        8,
        space=pl.ANY,
        scratch=[pltpu.SemaphoreType.DMA((4 + members + chips,))],
    )
    other = across(own)
    far = across(near)
    stored, gains, sent = call(
        functools.partial(dispatch_kernel, pack, experts, capacity),
        (
            shape((tok_rows, features), BF16),
            shape((chips, 8, width), F32),
            shape((experts * half, width), BF16),
        ),
        (near, far, own, *in_hbm(other), routes.T),
        2 * experts * half * width * tok_rows,
        16,
        space=(pltpu.VMEM, pltpu.VMEM, pltpu.VMEM, pl.ANY, pltpu.VMEM),
        scratch=[pltpu.VMEM((pack.rows - pack.project, width), BF16), pltpu.SemaphoreType.DMA(())],
    )
    x = lax.all_to_all(
        sent.reshape(experts, half, width), "sp", split_axis=0, concat_axis=0, tiled=True
    ).reshape(held, width)

    (fetched,) = call(
        fetch_kernel,
        (pltpu.VMEM((pack.project, width), BF16),),
        in_hbm(other),
        pack.rows * width * 512,
        8,
        space=pl.ANY,
        scratch=[pltpu.SemaphoreType.DMA(())],
    )
    packs = (own, fetched)
    acc_shape = (shape((held, 4 * units), F32), shape((held, 128), F32))
    chunk_flops = 2 * held * width * 4 * units
    acc, square = call(
        functools.partial(first_kernel, pack, chips), acc_shape, (x, gains, *packs), chunk_flops, 16
    )
    ahead, back = x, x
    last = chips // 2
    for step in range(1, last):
        ahead = along(ahead, 1)
        back = along(back, -1)
        acc, square = call(
            functools.partial(both_kernel, pack, chips, step),
            acc_shape,
            (ahead, back, gains, *packs, acc, square),
            2 * chunk_flops,
            16,
            {5: 0, 6: 1},
        )
    ahead = along(ahead, 1)
    _, _, hidden, ahead, back = call(
        functools.partial(last_kernel, pack, chips, float(total)),
        (*acc_shape, shape((held, CORES * units), BF16), *(shape((held, width), BF16),) * 2),
        (ahead, gains, *packs, acc, square),
        2 * chunk_flops,
        24,
        {4: 0, 5: 1},
    )

    def joined(part, came):
        return call(add_kernel, shape((held, width), BF16), (part, came), held * width, 8)

    steps = [*range(last - 1, -1, -1), *range(2 - last, 0)]
    parts = call(
        functools.partial(down_kernel, pack, chips, steps),
        (shape((held, width), F32),) * len(steps),
        (hidden, *packs),
        chunk_flops // 2 * len(steps),
        24,
    )
    part = dict(zip(steps, parts))
    for step in range(last - 1, -1, -1):
        ahead = along(ahead, 1, -1)
        if step:
            back = along(back, -1, -1)
            ahead = joined(part[step], ahead)
            back = joined(part[1 - step], back) if step > 1 else back
    result = call(own_kernel, pltpu.VMEM((held, width), BF16), (part[0], ahead, back), held * width, 8)
    returned = lax.all_to_all(
        result.reshape(blocks, half, width), "sp", split_axis=0, concat_axis=0, tiled=True
    ).reshape(experts * half, width)
    mine, theirs = call(
        functools.partial(pick_kernel, experts, capacity),
        (shape((tok_rows, features), F32),) * 2,
        (returned, routes.T, route_weight.T),
        4 * experts * half * width * tok_rows,
        12,
    )
    return call(
        join_kernel,
        shape((tok_rows, features), BF16),
        (stored, mine, across(theirs)),
        tok_rows * features,
        8,
    )


def solution(mesh):
    in_specs = (
        P("sp", "tp"),
        P("tp", None, None),
        P("tp"),
        P(None, "tp"),
        P("sp", "tp"),
        P("tp"),
        P("sp", None),
        P("sp", None),
        P("sp", None, "tp"),
        P("sp", None, "tp"),
        P("sp", "tp", None),
    )
    out_specs = P("sp", "tp")

    return jax.shard_map(on_device, mesh=mesh, in_specs=in_specs, out_specs=out_specs, check_vma=False)
```

```python
import functools

import jax
import jax.numpy as jnp
from jax import lax
from jax.experimental import pallas as pl
from jax.experimental.pallas import tpu as pltpu
from jax.sharding import PartitionSpec as P


GSIZE = 64
TOPK = 2
CORES = 2

GATE_LIMIT = 7.0
GATE_ALPHA = 1.702
NORM_EPS = 1e-05

F32 = jnp.float32
BF16 = jnp.bfloat16
MIB = 1024 * 1024


def iota(shape, dim):
    return lax.broadcasted_iota(jnp.int32, shape, dim)


def mm(a, b, ca=1, cb=0):
    return lax.dot_general(a, b, (((ca,), (cb,)), ((), ())), preferred_element_type=F32)


def call(kernel, out_shape, args, flops, mib, aliases=None, space=pltpu.VMEM, scratch=()):
    return pl.pallas_call(
        kernel,
        out_shape=out_shape,
        in_specs=[pl.BlockSpec(memory_space=space)] * len(args),
        scratch_shapes=scratch,
        out_specs=jax.tree.map(lambda _: pl.BlockSpec(memory_space=pltpu.VMEM), out_shape),
        compiler_params=pltpu.CompilerParams(vmem_limit_bytes=mib * MIB),
        cost_estimate=pl.CostEstimate(flops=flops, bytes_accessed=flops // 512, transcendentals=0),
        input_output_aliases=aliases or {},
    )(*args)


def pool_kernel(before_ref, x_ref, w_ref, gain_ref, norm_ref, out_ref):
    width, rows = x_ref.shape
    window = lax.shift_left(jnp.int32(2), lax.rem(lax.axis_index("tp"), 4))
    place = iota((rows, rows), 1) - iota((rows, rows), 0)
    inside = jnp.where((place >= 0) & (place < window), 1.0, 0.0).astype(BF16)
    reach = before_ref.shape[1]
    gap = iota((reach, rows), 1) + reach - iota((reach, rows), 0)
    behind = jnp.where(gap < window, 1.0, 0.0).astype(BF16)
    x = x_ref[...]
    total = mm(x, inside) + mm(before_ref[...], behind)
    spot = lax.axis_index("sp") * rows + iota((1, rows), 1)
    count = jnp.minimum(spot + 1, window).astype(F32)
    pooled = (total / count - x.astype(F32)).astype(BF16)
    eye = iota((width, width), 0) == iota((width, width), 1)
    gain = jnp.sum(jnp.where(eye, gain_ref[...].astype(F32), 0.0), axis=1, keepdims=True)
    out_ref[:width, :] = (mm(w_ref[...], pooled, 0, 0) * gain).astype(BF16)
    features = norm_ref.shape[1]
    tail = out_ref.shape[0] - width
    out_ref[width:, :features] = jnp.broadcast_to(norm_ref[...].astype(F32), (tail, features)).astype(BF16)
    out_ref[width:, features:] = jnp.zeros((tail, out_ref.shape[1] - features), BF16)


def row_slots(routes_ref, experts, capacity):
    rows = routes_ref.shape[1]
    named = [iota((experts, rows), 0) == routes_ref[k : k + 1, :] for k in range(TOPK)]
    ones = sum(jnp.where(n, 1.0, 0.0) for n in named)
    upper = jnp.where(iota((rows, rows), 0) < iota((rows, rows), 1), 1.0, 0.0).astype(BF16)
    earlier = mm(ones.astype(BF16), upper)
    slots = []
    for k in range(TOPK):
        rank = jnp.sum(jnp.where(named[k], earlier, 0.0), axis=0, keepdims=True).astype(jnp.int32)
        slots.append(routes_ref[k : k + 1, :] * capacity + rank)
    return slots


def slot_ids(shape, dim, capacity, core):
    half = capacity // CORES
    place = iota(shape, dim)
    return lax.div(place, half) * capacity + core * half + lax.rem(place, half)


class Pack:
    def __init__(self, deep, width, channels, rows):
        self.gate, self.up, self.down = 0, deep, 2 * deep
        self.project = 3 * deep
        self.resid = self.project + channels // 2
        self.rows = self.resid + rows // 2
        self.width = width


def prep_kernel(pack, gate, up, down, project, resid, x, w, gain, norm, out, x_out, w_out, gain_out, norm_out, sems):
    width, features = pack.width, project.shape[1]
    units = down.shape[0]
    pairs = [(x, x_out), (w, w_out), (gain, gain_out), (norm, norm_out)]
    for base, source in ((pack.project, project), (pack.resid, resid)):
        half = source.shape[0] // 2
        for i in range(2):
            pairs.append(
                (source.at[i * half : (i + 1) * half, :],
                 out.at[base : base + half, i * features : (i + 1) * features])
            )
    pairs.append((gate, out.at[pack.gate : pack.up, :]))
    pairs.append((up, out.at[pack.up : pack.down, :]))
    for i in range(down.shape[1] // width):
        pairs.append(
            (down.at[:, i * width : (i + 1) * width], out.at[pack.down + i * units : pack.down + (i + 1) * units, :])
        )
    copies = [pltpu.make_async_copy(a, b, sems.at[i]) for i, (a, b) in enumerate(pairs)]
    for copy in copies:
        copy.start()
    for copy in copies:
        copy.wait()


def dispatch_kernel(pack, experts, capacity, mixed_ref, own_ref, other_ref, routes_ref, stream_ref, gain_ref, out_ref):
    core = lax.rem(lax.axis_index("tp"), CORES)
    members, _, rows = mixed_ref.shape
    features = stream_ref.shape[1]
    mixed = mixed_ref[:, :GSIZE, :].reshape(members * GSIZE, rows)
    deep = members * GSIZE // 2
    streams = []
    for ref in (own_ref, other_ref):
        halves = [ref[pack.project : pack.resid, i * features : (i + 1) * features] for i in range(2)]
        projected = mm(mixed[:deep], halves[0], 0, 0) + mm(mixed[deep:], halves[1], 0, 0)
        resid = jnp.concatenate(
            [ref[pack.resid : pack.rows, i * features : (i + 1) * features] for i in range(2)], axis=0
        )
        streams.append((resid.astype(F32) + projected).astype(BF16))
    own, other = streams
    stream_ref[...] = own
    for t in range(members):
        y, c = divmod(t, CORES)
        gain_ref[y, :, c * features : (c + 1) * features] = mixed_ref[t, GSIZE : GSIZE + 8, :features].astype(F32)
    slots = row_slots(routes_ref, experts, capacity)
    ids = slot_ids((out_ref.shape[0], rows), 0, capacity, core)
    hit = (slots[0] == ids) | (slots[1] == ids)
    chosen = jnp.where(hit, 1.0, 0.0).astype(BF16)
    out_ref[:, :features] = mm(chosen, jnp.where(core == 0, own, other)).astype(BF16)
    out_ref[:, features:] = mm(chosen, jnp.where(core == 0, other, own)).astype(BF16)


def add_chunk(pack, x, chip, gain_ref, packs, acc_ref, square_ref, first=False):
    width = x.shape[1]
    value = x.astype(F32)
    square = value * value
    lanes = square_ref.shape[1]
    square = sum(square[:, i : i + lanes] for i in range(0, width, lanes))
    scaled = (value * gain_ref[chip, 0:1, :]).astype(BF16)
    for i, base in enumerate((pack.gate, pack.up)):
        for j, ref in enumerate(packs):
            rows = pl.ds(pl.multiple_of(base + chip * width, width), width)
            part = mm(scaled, ref[rows, :])
            columns = part.shape[1]
            span = slice((2 * i + j) * columns, (2 * i + j + 1) * columns)
            acc_ref[:, span] = part if first else acc_ref[:, span] + part
    square_ref[...] = square if first else square_ref[...] + square


def chip_at(chips, step):
    here = lax.div(lax.axis_index("tp"), CORES)
    return lax.rem(here + step + chips, chips)


def chip_across(chips, step):
    core = lax.rem(lax.axis_index("tp"), CORES)
    return chip_at(chips, step * (1 - 2 * core))


def first_kernel(pack, chips, x_ref, gain_ref, own_ref, other_ref, acc_ref, square_ref):
    add_chunk(pack, x_ref[...], chip_at(chips, 0), gain_ref, (own_ref, other_ref), acc_ref, square_ref, True)


def both_kernel(pack, chips, step, p_ref, m_ref, gain_ref, own_ref, other_ref, acc_in, square_in, acc_ref, square_ref):
    packs = (own_ref, other_ref)
    add_chunk(pack, p_ref[...], chip_at(chips, -step), gain_ref, packs, acc_ref, square_ref)
    add_chunk(pack, m_ref[...], chip_at(chips, step), gain_ref, packs, acc_ref, square_ref)


def partial(pack, hidden_ref, packs, chip):
    units = hidden_ref.shape[1] // CORES
    rows = pl.ds(pl.multiple_of(pack.down + chip * units, units), units)
    return sum(mm(hidden_ref[:, i * units : (i + 1) * units], ref[rows, :]) for i, ref in enumerate(packs))


def last_kernel(
    pack, chips, total, p_ref, m_ref, gain_ref, own_ref, other_ref, acc_in, square_in, acc_ref, square_ref, hidden_ref, up_ref, low_ref
):
    packs = (own_ref, other_ref)
    far = chip_at(chips, chips // 2)
    came = jnp.where(lax.rem(lax.axis_index("tp"), CORES) == 0, p_ref[...], m_ref[...])
    add_chunk(pack, came, far, gain_ref, packs, acc_ref, square_ref)
    mean = jnp.sum(square_ref[...], axis=1, keepdims=True) / total
    scale = lax.rsqrt(mean + NORM_EPS)
    units = hidden_ref.shape[1]
    gate = jnp.minimum(acc_ref[:, :units] * scale, GATE_LIMIT)
    up = jnp.clip(acc_ref[:, units:] * scale, -GATE_LIMIT, GATE_LIMIT)
    hidden_ref[...] = ((up + 1.0) * gate * jax.nn.sigmoid(GATE_ALPHA * gate)).astype(BF16)
    up_ref[...] = partial(pack, hidden_ref, packs, far).astype(BF16)
    low_ref[...] = partial(pack, hidden_ref, packs, chip_across(chips, 1 - chips // 2)).astype(BF16)


def down_kernel(pack, chips, steps, hidden_ref, own_ref, other_ref, *outs):
    for step, out_ref in zip(steps, outs):
        out_ref[...] = partial(pack, hidden_ref, (own_ref, other_ref), chip_across(chips, step))


def add_kernel(part_ref, came_ref, out_ref):
    out_ref[...] = (part_ref[...] + came_ref[...].astype(F32)).astype(BF16)


def own_kernel(part_ref, p_ref, m_ref, out_ref):
    out_ref[...] = (part_ref[...] + p_ref[...].astype(F32) + m_ref[...].astype(F32)).astype(BF16)


def pick_kernel(experts, capacity, back_ref, routes_ref, weight_ref, mine_ref, other_ref):
    core = lax.rem(lax.axis_index("tp"), CORES)
    slots = row_slots(routes_ref, experts, capacity)
    tokens = routes_ref.shape[1]
    ids = slot_ids((back_ref.shape[0], tokens), 0, capacity, core)
    eye = iota((tokens, tokens), 0) == iota((tokens, tokens), 1)
    rows = back_ref[...]
    total = 0.0
    for k in range(TOPK):
        chosen = jnp.where(slots[k] == ids, 1.0, 0.0).astype(BF16)
        weight = jnp.sum(jnp.where(eye, weight_ref[k : k + 1, :], 0.0), axis=1, keepdims=True)
        total = total + mm(chosen, rows, 0, 0) * weight
    features = mine_ref.shape[1]
    left, right = total[:, :features], total[:, features:]
    mine_ref[...] = jnp.where(core == 0, left, right)
    other_ref[...] = jnp.where(core == 0, right, left)


def join_kernel(stream_ref, mine_ref, other_ref, out_ref):
    out_ref[...] = (stream_ref[...].astype(F32) + mine_ref[...] + other_ref[...]).astype(BF16)


def on_device(
    pool_input,
    pool_weight,
    pool_gain,
    out_weight,
    resid,
    norm_gain,
    routes,
    route_weight,
    expert_gate,
    expert_up,
    expert_down,
):
    tok_rows, channels = pool_input.shape
    features = out_weight.shape[1]
    blocks, members = lax.axis_size("sp"), lax.axis_size("tp")
    chips = members // CORES
    experts = blocks * expert_gate.shape[0]
    capacity = 2 * tok_rows * TOPK // experts
    half = capacity // CORES
    width = features * CORES
    total = features * members
    held = blocks * half

    def along(value, step, other=1, cores=range(CORES)):
        steps = (step, step * other)
        pairs = [(y * CORES + c, (y + steps[c]) % chips * CORES + c) for y in range(chips) for c in cores]
        return lax.ppermute(value, "tp", pairs)

    def across(value):
        return lax.ppermute(value, "tp", [(t, t ^ 1) for t in range(members)])

    shape = jax.ShapeDtypeStruct
    deep, units = expert_gate.shape[1:]
    pack = Pack(deep, width, out_weight.shape[0], tok_rows)
    before = lax.ppermute(
        pool_input.T, "sp", [(s, s + 1) for s in range(blocks - 1)]
    )
    small = (pool_input.T, pool_weight[0], pool_gain.reshape(1, channels), norm_gain.reshape(1, features))
    own, *small = call(
        functools.partial(prep_kernel, pack),
        (pltpu.VMEM((pack.rows, width), BF16), *(pltpu.VMEM(v.shape, v.dtype) for v in small)),
        tuple(
            pltpu.with_memory_space_constraint(v, pltpu.HBM)
            for v in (expert_gate[0], expert_up[0], expert_down[0], out_weight, resid, *small)
        ),
        pack.rows * width * 512,
        8,
        space=pltpu.HBM,
        scratch=[pltpu.SemaphoreType.DMA((10 + chips,))],
    )
    other = across(own)
    packs = (own, other)
    pooled = call(
        pool_kernel,
        shape((GSIZE + 16, tok_rows), BF16),
        (before, *small),
        tok_rows * tok_rows * channels * 2,
        8,
    )
    mixed = lax.all_gather(pooled, "tp", axis=0, tiled=False)
    stored, gains, sent = call(
        functools.partial(dispatch_kernel, pack, experts, capacity),
        (
            shape((tok_rows, features), BF16),
            shape((chips, 8, width), F32),
            shape((experts * half, width), BF16),
        ),
        (mixed, *packs, routes.T),
        2 * experts * half * width * tok_rows,
        16,
    )
    x = lax.all_to_all(
        sent.reshape(experts, half, width), "sp", split_axis=0, concat_axis=0, tiled=True
    ).reshape(held, width)

    acc_shape = (shape((held, 4 * units), F32), shape((held, 128), F32))
    chunk_flops = 2 * held * width * 4 * units
    acc, square = call(
        functools.partial(first_kernel, pack, chips), acc_shape, (x, gains, *packs), chunk_flops, 16
    )
    ahead, back = x, x
    last = chips // 2
    for step in range(1, last):
        ahead = along(ahead, 1)
        back = along(back, -1)
        acc, square = call(
            functools.partial(both_kernel, pack, chips, step),
            acc_shape,
            (ahead, back, gains, *packs, acc, square),
            2 * chunk_flops,
            16,
            {5: 0, 6: 1},
        )
    ahead = along(ahead, 1, cores=(0,))
    back = along(back, -1, cores=(1,))
    _, _, hidden, ahead, back = call(
        functools.partial(last_kernel, pack, chips, float(total)),
        (*acc_shape, shape((held, CORES * units), BF16), *(shape((held, width), BF16),) * 2),
        (ahead, back, gains, *packs, acc, square),
        2 * chunk_flops,
        24,
        {5: 0, 6: 1},
    )

    def joined(part, came):
        return call(add_kernel, shape((held, width), BF16), (part, came), held * width, 8)

    steps = [*range(last - 1, -1, -1), *range(2 - last, 0)]
    parts = call(
        functools.partial(down_kernel, pack, chips, steps),
        (shape((held, width), F32),) * len(steps),
        (hidden, *packs),
        chunk_flops // 2 * len(steps),
        24,
    )
    part = dict(zip(steps, parts))
    for step in range(last - 1, -1, -1):
        ahead = along(ahead, 1, -1)
        if step:
            back = along(back, -1, -1)
            ahead = joined(part[step], ahead)
            back = joined(part[1 - step], back) if step > 1 else back
    result = call(own_kernel, pltpu.VMEM((held, width), BF16), (part[0], ahead, back), held * width, 8)
    returned = lax.all_to_all(
        result.reshape(blocks, half, width), "sp", split_axis=0, concat_axis=0, tiled=True
    ).reshape(experts * half, width)
    mine, theirs = call(
        functools.partial(pick_kernel, experts, capacity),
        (shape((tok_rows, features), F32),) * 2,
        (returned, routes.T, route_weight.T),
        4 * experts * half * width * tok_rows,
        12,
    )
    return call(
        join_kernel,
        shape((tok_rows, features), BF16),
        (stored, mine, across(theirs)),
        tok_rows * features,
        8,
    )


def solution(mesh):
    in_specs = (
        P("sp", "tp"),
        P("tp", None, None),
        P("tp"),
        P(None, "tp"),
        P("sp", "tp"),
        P("tp"),
        P("sp", None),
        P("sp", None),
        P("sp", None, "tp"),
        P("sp", None, "tp"),
        P("sp", "tp", None),
    )
    out_specs = P("sp", "tp")

    return jax.shard_map(on_device, mesh=mesh, in_specs=in_specs, out_specs=out_specs, check_vma=False)
```

```python
import functools

import jax
import jax.numpy as jnp
from jax import lax
from jax.experimental import pallas as pl
from jax.experimental.pallas import tpu as pltpu
from jax.sharding import PartitionSpec as P


GSIZE = 64
TOPK = 2
CORES = 2

GATE_LIMIT = 7.0
GATE_ALPHA = 1.702
NORM_EPS = 1e-05

F32 = jnp.float32
BF16 = jnp.bfloat16
MIB = 1024 * 1024


def iota(shape, dim):
    return lax.broadcasted_iota(jnp.int32, shape, dim)


def mm(a, b, ca=1, cb=0):
    return lax.dot_general(a, b, (((ca,), (cb,)), ((), ())), preferred_element_type=F32)


def call(kernel, out_shape, args, flops, mib, aliases=None, space=pltpu.VMEM, scratch=()):
    return pl.pallas_call(
        kernel,
        out_shape=out_shape,
        in_specs=[pl.BlockSpec(memory_space=space)] * len(args),
        scratch_shapes=scratch,
        out_specs=jax.tree.map(lambda _: pl.BlockSpec(memory_space=pltpu.VMEM), out_shape),
        compiler_params=pltpu.CompilerParams(vmem_limit_bytes=mib * MIB),
        cost_estimate=pl.CostEstimate(flops=flops, bytes_accessed=flops // 512, transcendentals=0),
        input_output_aliases=aliases or {},
    )(*args)


def pool_kernel(before_ref, x_ref, w_ref, gain_ref, norm_ref, out_ref):
    width, rows = x_ref.shape
    window = lax.shift_left(jnp.int32(2), lax.rem(lax.axis_index("tp"), 4))
    place = iota((rows, rows), 1) - iota((rows, rows), 0)
    inside = jnp.where((place >= 0) & (place < window), 1.0, 0.0).astype(BF16)
    reach = before_ref.shape[1]
    gap = iota((reach, rows), 1) + reach - iota((reach, rows), 0)
    behind = jnp.where(gap < window, 1.0, 0.0).astype(BF16)
    x = x_ref[...]
    total = mm(x, inside) + mm(before_ref[...], behind)
    spot = lax.axis_index("sp") * rows + iota((1, rows), 1)
    count = jnp.minimum(spot + 1, window).astype(F32)
    pooled = (total / count - x.astype(F32)).astype(BF16)
    eye = iota((width, width), 0) == iota((width, width), 1)
    gain = jnp.sum(jnp.where(eye, gain_ref[...].astype(F32), 0.0), axis=1, keepdims=True)
    out_ref[:width, :] = (mm(w_ref[...], pooled, 0, 0) * gain).astype(BF16)
    features = norm_ref.shape[1]
    tail = out_ref.shape[0] - width
    out_ref[width:, :features] = jnp.broadcast_to(norm_ref[...].astype(F32), (tail, features)).astype(BF16)
    out_ref[width:, features:] = jnp.zeros((tail, out_ref.shape[1] - features), BF16)


def row_slots(routes_ref, experts, capacity):
    rows = routes_ref.shape[1]
    named = [iota((experts, rows), 0) == routes_ref[k : k + 1, :] for k in range(TOPK)]
    ones = sum(jnp.where(n, 1.0, 0.0) for n in named)
    upper = jnp.where(iota((rows, rows), 0) < iota((rows, rows), 1), 1.0, 0.0).astype(BF16)
    earlier = mm(ones.astype(BF16), upper)
    slots = []
    for k in range(TOPK):
        rank = jnp.sum(jnp.where(named[k], earlier, 0.0), axis=0, keepdims=True).astype(jnp.int32)
        slots.append(routes_ref[k : k + 1, :] * capacity + rank)
    return slots


def slot_ids(shape, dim, capacity, core):
    half = capacity // CORES
    place = iota(shape, dim)
    return lax.div(place, half) * capacity + core * half + lax.rem(place, half)


class Pack:
    def __init__(self, deep, width, channels, rows):
        self.gate, self.up, self.down, self.weights = 0, deep, 2 * deep, 3 * deep
        self.project, self.resid, self.rows = 0, channels // 2, (channels + rows) // 2
        self.width = width


def copy_all(pairs, sems):
    copies = [pltpu.make_async_copy(a, b, sems.at[i]) for i, (a, b) in enumerate(pairs)]
    for copy in copies:
        copy.start()
    for copy in copies:
        copy.wait()


def prep_kernel(pack, project, resid, x, w, gain, norm, out, x_out, w_out, gain_out, norm_out, sems):
    features = project.shape[1]
    pairs = [(x, x_out), (w, w_out), (gain, gain_out), (norm, norm_out)]
    for base, source in ((pack.project, project), (pack.resid, resid)):
        half = source.shape[0] // 2
        for i in range(2):
            pairs.append(
                (source.at[i * half : (i + 1) * half, :],
                 out.at[base : base + half, i * features : (i + 1) * features])
            )
    copy_all(pairs, sems)


def weights_kernel(pack, gate, up, down, out, sems):
    width, units = pack.width, down.shape[0]
    pairs = [(gate, out.at[pack.gate : pack.up, :]), (up, out.at[pack.up : pack.down, :])]
    for i in range(down.shape[1] // width):
        pairs.append(
            (down.at[:, i * width : (i + 1) * width], out.at[pack.down + i * units : pack.down + (i + 1) * units, :])
        )
    copy_all(pairs, sems)


def dispatch_kernel(pack, experts, capacity, mixed_ref, own_ref, other_ref, routes_ref, stream_ref, gain_ref, out_ref):
    core = lax.rem(lax.axis_index("tp"), CORES)
    members, _, rows = mixed_ref.shape
    features = stream_ref.shape[1]
    mixed = mixed_ref[:, :GSIZE, :].reshape(members * GSIZE, rows)
    deep = members * GSIZE // 2
    streams = []
    for ref in (own_ref, other_ref):
        halves = [ref[pack.project : pack.resid, i * features : (i + 1) * features] for i in range(2)]
        projected = mm(mixed[:deep], halves[0], 0, 0) + mm(mixed[deep:], halves[1], 0, 0)
        resid = jnp.concatenate(
            [ref[pack.resid : pack.rows, i * features : (i + 1) * features] for i in range(2)], axis=0
        )
        streams.append((resid.astype(F32) + projected).astype(BF16))
    own, other = streams
    stream_ref[...] = own
    for t in range(members):
        y, c = divmod(t, CORES)
        gain_ref[y, :, c * features : (c + 1) * features] = mixed_ref[t, GSIZE : GSIZE + 8, :features].astype(F32)
    slots = row_slots(routes_ref, experts, capacity)
    ids = slot_ids((out_ref.shape[0], rows), 0, capacity, core)
    hit = (slots[0] == ids) | (slots[1] == ids)
    chosen = jnp.where(hit, 1.0, 0.0).astype(BF16)
    out_ref[:, :features] = mm(chosen, jnp.where(core == 0, own, other)).astype(BF16)
    out_ref[:, features:] = mm(chosen, jnp.where(core == 0, other, own)).astype(BF16)


def add_chunk(pack, x, chip, gain_ref, packs, acc_ref, square_ref, first=False):
    width = x.shape[1]
    value = x.astype(F32)
    square = value * value
    lanes = square_ref.shape[1]
    square = sum(square[:, i : i + lanes] for i in range(0, width, lanes))
    scaled = (value * gain_ref[chip, 0:1, :]).astype(BF16)
    for i, base in enumerate((pack.gate, pack.up)):
        for j, ref in enumerate(packs):
            rows = pl.ds(pl.multiple_of(base + chip * width, width), width)
            part = mm(scaled, ref[rows, :])
            columns = part.shape[1]
            span = slice((2 * i + j) * columns, (2 * i + j + 1) * columns)
            acc_ref[:, span] = part if first else acc_ref[:, span] + part
    square_ref[...] = square if first else square_ref[...] + square


def chip_at(chips, step):
    here = lax.div(lax.axis_index("tp"), CORES)
    return lax.rem(here + step + chips, chips)


def chip_across(chips, step):
    core = lax.rem(lax.axis_index("tp"), CORES)
    return chip_at(chips, step * (1 - 2 * core))


def first_kernel(pack, chips, x_ref, gain_ref, own_ref, other_ref, acc_ref, square_ref):
    add_chunk(pack, x_ref[...], chip_at(chips, 0), gain_ref, (own_ref, other_ref), acc_ref, square_ref, True)


def both_kernel(pack, chips, step, p_ref, m_ref, gain_ref, own_ref, other_ref, acc_in, square_in, acc_ref, square_ref):
    packs = (own_ref, other_ref)
    add_chunk(pack, p_ref[...], chip_at(chips, -step), gain_ref, packs, acc_ref, square_ref)
    add_chunk(pack, m_ref[...], chip_at(chips, step), gain_ref, packs, acc_ref, square_ref)


def partial(pack, hidden_ref, packs, chip):
    units = hidden_ref.shape[1] // CORES
    rows = pl.ds(pl.multiple_of(pack.down + chip * units, units), units)
    return sum(mm(hidden_ref[:, i * units : (i + 1) * units], ref[rows, :]) for i, ref in enumerate(packs))


def last_kernel(
    pack, chips, total, p_ref, gain_ref, own_ref, other_ref, acc_in, square_in, acc_ref, square_ref, hidden_ref, up_ref, low_ref
):
    packs = (own_ref, other_ref)
    far = chip_at(chips, chips // 2)
    add_chunk(pack, p_ref[...], far, gain_ref, packs, acc_ref, square_ref)
    mean = jnp.sum(square_ref[...], axis=1, keepdims=True) / total
    scale = lax.rsqrt(mean + NORM_EPS)
    units = hidden_ref.shape[1]
    gate = jnp.minimum(acc_ref[:, :units] * scale, GATE_LIMIT)
    up = jnp.clip(acc_ref[:, units:] * scale, -GATE_LIMIT, GATE_LIMIT)
    hidden_ref[...] = ((up + 1.0) * gate * jax.nn.sigmoid(GATE_ALPHA * gate)).astype(BF16)
    up_ref[...] = partial(pack, hidden_ref, packs, far).astype(BF16)
    low_ref[...] = partial(pack, hidden_ref, packs, chip_across(chips, 1 - chips // 2)).astype(BF16)


def down_kernel(pack, chips, steps, hidden_ref, own_ref, other_ref, *outs):
    for step, out_ref in zip(steps, outs):
        out_ref[...] = partial(pack, hidden_ref, (own_ref, other_ref), chip_across(chips, step))


def add_kernel(part_ref, came_ref, out_ref):
    out_ref[...] = (part_ref[...] + came_ref[...].astype(F32)).astype(BF16)


def own_kernel(part_ref, p_ref, m_ref, out_ref):
    out_ref[...] = (part_ref[...] + p_ref[...].astype(F32) + m_ref[...].astype(F32)).astype(BF16)


def pick_kernel(experts, capacity, back_ref, routes_ref, weight_ref, mine_ref, other_ref):
    core = lax.rem(lax.axis_index("tp"), CORES)
    slots = row_slots(routes_ref, experts, capacity)
    tokens = routes_ref.shape[1]
    ids = slot_ids((back_ref.shape[0], tokens), 0, capacity, core)
    eye = iota((tokens, tokens), 0) == iota((tokens, tokens), 1)
    rows = back_ref[...]
    total = 0.0
    for k in range(TOPK):
        chosen = jnp.where(slots[k] == ids, 1.0, 0.0).astype(BF16)
        weight = jnp.sum(jnp.where(eye, weight_ref[k : k + 1, :], 0.0), axis=1, keepdims=True)
        total = total + mm(chosen, rows, 0, 0) * weight
    features = mine_ref.shape[1]
    left, right = total[:, :features], total[:, features:]
    mine_ref[...] = jnp.where(core == 0, left, right)
    other_ref[...] = jnp.where(core == 0, right, left)


def join_kernel(stream_ref, mine_ref, other_ref, out_ref):
    out_ref[...] = (stream_ref[...].astype(F32) + mine_ref[...] + other_ref[...]).astype(BF16)


def on_device(
    pool_input,
    pool_weight,
    pool_gain,
    out_weight,
    resid,
    norm_gain,
    routes,
    route_weight,
    expert_gate,
    expert_up,
    expert_down,
):
    tok_rows, channels = pool_input.shape
    features = out_weight.shape[1]
    blocks, members = lax.axis_size("sp"), lax.axis_size("tp")
    chips = members // CORES
    experts = blocks * expert_gate.shape[0]
    capacity = 2 * tok_rows * TOPK // experts
    half = capacity // CORES
    width = features * CORES
    total = features * members
    held = blocks * half

    def along(value, step, other=1):
        pairs = [(y * CORES, (y + step) % chips * CORES) for y in range(chips)]
        pairs += [(y * CORES + 1, (y + step * other) % chips * CORES + 1) for y in range(chips)]
        return lax.ppermute(value, "tp", pairs)

    def across(value):
        return lax.ppermute(value, "tp", [(t, t ^ 1) for t in range(members)])

    shape = jax.ShapeDtypeStruct
    deep, units = expert_gate.shape[1:]
    pack = Pack(deep, width, out_weight.shape[0], tok_rows)

    def in_hbm(*values):
        return tuple(pltpu.with_memory_space_constraint(v, pltpu.HBM) for v in values)

    before = lax.ppermute(
        pool_input.T, "sp", [(s, s + 1) for s in range(blocks - 1)]
    )
    small = (pool_input.T, pool_weight[0], pool_gain.reshape(1, channels), norm_gain.reshape(1, features))
    own, *small = call(
        functools.partial(prep_kernel, pack),
        (pltpu.VMEM((pack.rows, width), BF16), *(pltpu.VMEM(v.shape, v.dtype) for v in small)),
        in_hbm(out_weight, resid, *small),
        pack.rows * width * 512,
        8,
        space=pl.ANY,
        scratch=[pltpu.SemaphoreType.DMA((8,))],
    )
    other = across(own)
    pooled = call(
        pool_kernel,
        shape((GSIZE + 16, tok_rows), BF16),
        (before, *small),
        tok_rows * tok_rows * channels * 2,
        8,
    )
    mixed = lax.all_gather(pooled, "tp", axis=0, tiled=False)
    stored, gains, sent = call(
        functools.partial(dispatch_kernel, pack, experts, capacity),
        (
            shape((tok_rows, features), BF16),
            shape((chips, 8, width), F32),
            shape((experts * half, width), BF16),
        ),
        (mixed, own, other, routes.T),
        2 * experts * half * width * tok_rows,
        16,
    )
    x = lax.all_to_all(
        sent.reshape(experts, half, width), "sp", split_axis=0, concat_axis=0, tiled=True
    ).reshape(held, width)

    (own,) = call(
        functools.partial(weights_kernel, pack),
        (pltpu.VMEM((pack.weights, width), BF16),),
        in_hbm(expert_gate[0], expert_up[0], expert_down[0]),
        pack.weights * width * 512,
        8,
        space=pl.ANY,
        scratch=[pltpu.SemaphoreType.DMA((2 + chips,))],
    )
    packs = (own, across(own))
    acc_shape = (shape((held, 4 * units), F32), shape((held, 128), F32))
    chunk_flops = 2 * held * width * 4 * units
    acc, square = call(
        functools.partial(first_kernel, pack, chips), acc_shape, (x, gains, *packs), chunk_flops, 16
    )
    ahead, back = x, x
    last = chips // 2
    for step in range(1, last):
        ahead = along(ahead, 1)
        back = along(back, -1)
        acc, square = call(
            functools.partial(both_kernel, pack, chips, step),
            acc_shape,
            (ahead, back, gains, *packs, acc, square),
            2 * chunk_flops,
            16,
            {5: 0, 6: 1},
        )
    ahead = along(ahead, 1)
    _, _, hidden, ahead, back = call(
        functools.partial(last_kernel, pack, chips, float(total)),
        (*acc_shape, shape((held, CORES * units), BF16), *(shape((held, width), BF16),) * 2),
        (ahead, gains, *packs, acc, square),
        2 * chunk_flops,
        24,
        {4: 0, 5: 1},
    )

    def joined(part, came):
        return call(add_kernel, shape((held, width), BF16), (part, came), held * width, 8)

    steps = [*range(last - 1, -1, -1), *range(2 - last, 0)]
    parts = call(
        functools.partial(down_kernel, pack, chips, steps),
        (shape((held, width), F32),) * len(steps),
        (hidden, *packs),
        chunk_flops // 2 * len(steps),
        24,
    )
    part = dict(zip(steps, parts))
    for step in range(last - 1, -1, -1):
        ahead = along(ahead, 1, -1)
        if step:
            back = along(back, -1, -1)
            ahead = joined(part[step], ahead)
            back = joined(part[1 - step], back) if step > 1 else back
    result = call(own_kernel, pltpu.VMEM((held, width), BF16), (part[0], ahead, back), held * width, 8)
    returned = lax.all_to_all(
        result.reshape(blocks, half, width), "sp", split_axis=0, concat_axis=0, tiled=True
    ).reshape(experts * half, width)
    mine, theirs = call(
        functools.partial(pick_kernel, experts, capacity),
        (shape((tok_rows, features), F32),) * 2,
        (returned, routes.T, route_weight.T),
        4 * experts * half * width * tok_rows,
        12,
    )
    return call(
        join_kernel,
        shape((tok_rows, features), BF16),
        (stored, mine, across(theirs)),
        tok_rows * features,
        8,
    )


def solution(mesh):
    in_specs = (
        P("sp", "tp"),
        P("tp", None, None),
        P("tp"),
        P(None, "tp"),
        P("sp", "tp"),
        P("tp"),
        P("sp", None),
        P("sp", None),
        P("sp", None, "tp"),
        P("sp", None, "tp"),
        P("sp", "tp", None),
    )
    out_specs = P("sp", "tp")

    return jax.shard_map(on_device, mesh=mesh, in_specs=in_specs, out_specs=out_specs, check_vma=False)
```

```python
import functools

import jax
import jax.numpy as jnp
from jax import lax
from jax.experimental import pallas as pl
from jax.experimental.pallas import tpu as pltpu
from jax.sharding import PartitionSpec as P


GSIZE = 64
TOPK = 2
CORES = 2

GATE_LIMIT = 7.0
GATE_ALPHA = 1.702
NORM_EPS = 1e-05

F32 = jnp.float32
BF16 = jnp.bfloat16
MIB = 1024 * 1024


def iota(shape, dim):
    return lax.broadcasted_iota(jnp.int32, shape, dim)


def mm(a, b, ca=1, cb=0):
    return lax.dot_general(a, b, (((ca,), (cb,)), ((), ())), preferred_element_type=F32)


def call(kernel, out_shape, args, flops, mib, aliases=None, space=pltpu.VMEM, scratch=()):
    return pl.pallas_call(
        kernel,
        out_shape=out_shape,
        in_specs=[pl.BlockSpec(memory_space=space)] * len(args),
        scratch_shapes=scratch,
        out_specs=jax.tree.map(lambda _: pl.BlockSpec(memory_space=pltpu.VMEM), out_shape),
        compiler_params=pltpu.CompilerParams(vmem_limit_bytes=mib * MIB),
        cost_estimate=pl.CostEstimate(flops=flops, bytes_accessed=flops // 512, transcendentals=0),
        input_output_aliases=aliases or {},
    )(*args)


def pool_kernel(before_ref, x_ref, w_ref, gain_ref, norm_ref, out_ref):
    width, rows = x_ref.shape
    window = lax.shift_left(jnp.int32(2), lax.rem(lax.axis_index("tp"), 4))
    place = iota((rows, rows), 1) - iota((rows, rows), 0)
    inside = jnp.where((place >= 0) & (place < window), 1.0, 0.0).astype(BF16)
    reach = before_ref.shape[1]
    gap = iota((reach, rows), 1) + reach - iota((reach, rows), 0)
    behind = jnp.where(gap < window, 1.0, 0.0).astype(BF16)
    x = x_ref[...]
    total = mm(x, inside) + mm(before_ref[...], behind)
    spot = lax.axis_index("sp") * rows + iota((1, rows), 1)
    count = jnp.minimum(spot + 1, window).astype(F32)
    pooled = (total / count - x.astype(F32)).astype(BF16)
    eye = iota((width, width), 0) == iota((width, width), 1)
    gain = jnp.sum(jnp.where(eye, gain_ref[...].astype(F32), 0.0), axis=1, keepdims=True)
    out_ref[:width, :] = (mm(w_ref[...], pooled, 0, 0) * gain).astype(BF16)
    features = norm_ref.shape[1]
    tail = out_ref.shape[0] - width
    out_ref[width:, :features] = jnp.broadcast_to(norm_ref[...].astype(F32), (tail, features)).astype(BF16)
    out_ref[width:, features:] = jnp.zeros((tail, out_ref.shape[1] - features), BF16)


def row_slots(routes_ref, experts, capacity):
    rows = routes_ref.shape[1]
    named = [iota((experts, rows), 0) == routes_ref[k : k + 1, :] for k in range(TOPK)]
    ones = sum(jnp.where(n, 1.0, 0.0) for n in named)
    upper = jnp.where(iota((rows, rows), 0) < iota((rows, rows), 1), 1.0, 0.0).astype(BF16)
    earlier = mm(ones.astype(BF16), upper)
    slots = []
    for k in range(TOPK):
        rank = jnp.sum(jnp.where(named[k], earlier, 0.0), axis=0, keepdims=True).astype(jnp.int32)
        slots.append(routes_ref[k : k + 1, :] * capacity + rank)
    return slots


def slot_ids(shape, dim, capacity, core):
    half = capacity // CORES
    place = iota(shape, dim)
    return lax.div(place, half) * capacity + core * half + lax.rem(place, half)


class Pack:
    def __init__(self, deep, width, channels, rows):
        self.gate, self.up, self.down = 0, deep, 2 * deep
        self.project = 3 * deep
        self.resid = self.project + channels // 2
        self.rows = self.resid + rows // 2
        self.width = width


def prep_kernel(pack, gate, up, down, project, resid, x, w, gain, norm, out, x_out, w_out, gain_out, norm_out, sems):
    width, features = pack.width, project.shape[1]
    units = down.shape[0]
    pairs = [(x, x_out), (w, w_out), (gain, gain_out), (norm, norm_out)]
    for base, source in ((pack.project, project), (pack.resid, resid)):
        half = source.shape[0] // 2
        for i in range(2):
            pairs.append(
                (source.at[i * half : (i + 1) * half, :],
                 out.at[base : base + half, i * features : (i + 1) * features])
            )
    pairs.append((gate, out.at[pack.gate : pack.up, :]))
    pairs.append((up, out.at[pack.up : pack.down, :]))
    for i in range(down.shape[1] // width):
        pairs.append(
            (down.at[:, i * width : (i + 1) * width], out.at[pack.down + i * units : pack.down + (i + 1) * units, :])
        )
    copies = [pltpu.make_async_copy(a, b, sems.at[i]) for i, (a, b) in enumerate(pairs)]
    for copy in copies:
        copy.start()
    for copy in copies:
        copy.wait()


def dispatch_kernel(pack, experts, capacity, mixed_ref, own_ref, other_ref, routes_ref, stream_ref, gain_ref, out_ref):
    core = lax.rem(lax.axis_index("tp"), CORES)
    members, _, rows = mixed_ref.shape
    features = stream_ref.shape[1]
    mixed = mixed_ref[:, :GSIZE, :].reshape(members * GSIZE, rows)
    deep = members * GSIZE // 2
    streams = []
    for ref in (own_ref, other_ref):
        halves = [ref[pack.project : pack.resid, i * features : (i + 1) * features] for i in range(2)]
        projected = mm(mixed[:deep], halves[0], 0, 0) + mm(mixed[deep:], halves[1], 0, 0)
        resid = jnp.concatenate(
            [ref[pack.resid : pack.rows, i * features : (i + 1) * features] for i in range(2)], axis=0
        )
        streams.append((resid.astype(F32) + projected).astype(BF16))
    own, other = streams
    stream_ref[...] = own
    for t in range(members):
        y, c = divmod(t, CORES)
        gain_ref[y, :, c * features : (c + 1) * features] = mixed_ref[t, GSIZE : GSIZE + 8, :features].astype(F32)
    slots = row_slots(routes_ref, experts, capacity)
    ids = slot_ids((out_ref.shape[0], rows), 0, capacity, core)
    hit = (slots[0] == ids) | (slots[1] == ids)
    chosen = jnp.where(hit, 1.0, 0.0).astype(BF16)
    out_ref[:, :features] = mm(chosen, jnp.where(core == 0, own, other)).astype(BF16)
    out_ref[:, features:] = mm(chosen, jnp.where(core == 0, other, own)).astype(BF16)


def add_chunk(pack, x, chip, gain_ref, packs, acc_ref, square_ref, first=False):
    width = x.shape[1]
    value = x.astype(F32)
    square = value * value
    lanes = square_ref.shape[1]
    square = sum(square[:, i : i + lanes] for i in range(0, width, lanes))
    scaled = (value * gain_ref[chip, 0:1, :]).astype(BF16)
    for i, base in enumerate((pack.gate, pack.up)):
        for j, ref in enumerate(packs):
            rows = pl.ds(pl.multiple_of(base + chip * width, width), width)
            part = mm(scaled, ref[rows, :])
            columns = part.shape[1]
            span = slice((2 * i + j) * columns, (2 * i + j + 1) * columns)
            acc_ref[:, span] = part if first else acc_ref[:, span] + part
    square_ref[...] = square if first else square_ref[...] + square


def chip_at(chips, step):
    here = lax.div(lax.axis_index("tp"), CORES)
    return lax.rem(here + step + chips, chips)


def chip_across(chips, step):
    core = lax.rem(lax.axis_index("tp"), CORES)
    return chip_at(chips, step * (2 * core - 1))


def first_kernel(pack, chips, x_ref, gain_ref, own_ref, other_ref, acc_ref, square_ref):
    add_chunk(pack, x_ref[...], chip_at(chips, 0), gain_ref, (own_ref, other_ref), acc_ref, square_ref, True)


def both_kernel(pack, chips, step, p_ref, m_ref, gain_ref, own_ref, other_ref, acc_in, square_in, acc_ref, square_ref):
    packs = (own_ref, other_ref)
    add_chunk(pack, p_ref[...], chip_at(chips, -step), gain_ref, packs, acc_ref, square_ref)
    add_chunk(pack, m_ref[...], chip_at(chips, step), gain_ref, packs, acc_ref, square_ref)


def partial(pack, hidden_ref, packs, chip):
    units = hidden_ref.shape[1] // CORES
    rows = pl.ds(pl.multiple_of(pack.down + chip * units, units), units)
    return sum(mm(hidden_ref[:, i * units : (i + 1) * units], ref[rows, :]) for i, ref in enumerate(packs))


def last_kernel(
    pack, chips, total, p_ref, gain_ref, own_ref, other_ref, acc_in, square_in, acc_ref, square_ref, hidden_ref, up_ref, low_ref
):
    packs = (own_ref, other_ref)
    far = chip_at(chips, chips // 2)
    add_chunk(pack, p_ref[...], far, gain_ref, packs, acc_ref, square_ref)
    mean = jnp.sum(square_ref[...], axis=1, keepdims=True) / total
    scale = lax.rsqrt(mean + NORM_EPS)
    units = hidden_ref.shape[1]
    gate = jnp.minimum(acc_ref[:, :units] * scale, GATE_LIMIT)
    up = jnp.clip(acc_ref[:, units:] * scale, -GATE_LIMIT, GATE_LIMIT)
    hidden_ref[...] = ((up + 1.0) * gate * jax.nn.sigmoid(GATE_ALPHA * gate)).astype(BF16)
    up_ref[...] = partial(pack, hidden_ref, packs, far).astype(BF16)
    low_ref[...] = partial(pack, hidden_ref, packs, chip_across(chips, 1 - chips // 2)).astype(BF16)


def down_kernel(pack, chips, steps, hidden_ref, own_ref, other_ref, *outs):
    for step, out_ref in zip(steps, outs):
        out_ref[...] = partial(pack, hidden_ref, (own_ref, other_ref), chip_across(chips, step))


def add_kernel(part_ref, came_ref, out_ref):
    out_ref[...] = (part_ref[...] + came_ref[...].astype(F32)).astype(BF16)


def own_kernel(part_ref, p_ref, m_ref, out_ref):
    out_ref[...] = (part_ref[...] + p_ref[...].astype(F32) + m_ref[...].astype(F32)).astype(BF16)


def pick_kernel(experts, capacity, back_ref, routes_ref, weight_ref, mine_ref, other_ref):
    core = lax.rem(lax.axis_index("tp"), CORES)
    slots = row_slots(routes_ref, experts, capacity)
    tokens = routes_ref.shape[1]
    ids = slot_ids((back_ref.shape[0], tokens), 0, capacity, core)
    eye = iota((tokens, tokens), 0) == iota((tokens, tokens), 1)
    rows = back_ref[...]
    total = 0.0
    for k in range(TOPK):
        chosen = jnp.where(slots[k] == ids, 1.0, 0.0).astype(BF16)
        weight = jnp.sum(jnp.where(eye, weight_ref[k : k + 1, :], 0.0), axis=1, keepdims=True)
        total = total + mm(chosen, rows, 0, 0) * weight
    features = mine_ref.shape[1]
    left, right = total[:, :features], total[:, features:]
    mine_ref[...] = jnp.where(core == 0, left, right)
    other_ref[...] = jnp.where(core == 0, right, left)


def join_kernel(stream_ref, mine_ref, other_ref, out_ref):
    out_ref[...] = (stream_ref[...].astype(F32) + mine_ref[...] + other_ref[...]).astype(BF16)


def on_device(
    pool_input,
    pool_weight,
    pool_gain,
    out_weight,
    resid,
    norm_gain,
    routes,
    route_weight,
    expert_gate,
    expert_up,
    expert_down,
):
    tok_rows, channels = pool_input.shape
    features = out_weight.shape[1]
    blocks, members = lax.axis_size("sp"), lax.axis_size("tp")
    chips = members // CORES
    experts = blocks * expert_gate.shape[0]
    capacity = 2 * tok_rows * TOPK // experts
    half = capacity // CORES
    width = features * CORES
    total = features * members
    held = blocks * half

    def along(value, step, other=1):
        pairs = [(y * CORES, (y + step) % chips * CORES) for y in range(chips)]
        pairs += [(y * CORES + 1, (y + step * other) % chips * CORES + 1) for y in range(chips)]
        return lax.ppermute(value, "tp", pairs)

    def across(value):
        return lax.ppermute(value, "tp", [(t, t ^ 1) for t in range(members)])

    shape = jax.ShapeDtypeStruct
    deep, units = expert_gate.shape[1:]
    pack = Pack(deep, width, out_weight.shape[0], tok_rows)
    before = lax.ppermute(
        pool_input.T, "sp", [(s, s + 1) for s in range(blocks - 1)]
    )
    small = (pool_input.T, pool_weight[0], pool_gain.reshape(1, channels), norm_gain.reshape(1, features))
    own, *small = call(
        functools.partial(prep_kernel, pack),
        (pltpu.VMEM((pack.rows, width), BF16), *(pltpu.VMEM(v.shape, v.dtype) for v in small)),
        tuple(
            pltpu.with_memory_space_constraint(v, pltpu.HBM)
            for v in (expert_gate[0], expert_up[0], expert_down[0], out_weight, resid, *small)
        ),
        pack.rows * width * 512,
        8,
        space=pltpu.HBM,
        scratch=[pltpu.SemaphoreType.DMA((10 + chips,))],
    )
    other = across(own)
    packs = (own, other)
    pooled = call(
        pool_kernel,
        shape((GSIZE + 16, tok_rows), BF16),
        (before, *small),
        tok_rows * tok_rows * channels * 2,
        8,
    )
    mixed = lax.all_gather(pooled, "tp", axis=0, tiled=False)
    stored, gains, sent = call(
        functools.partial(dispatch_kernel, pack, experts, capacity),
        (
            shape((tok_rows, features), BF16),
            shape((chips, 8, width), F32),
            shape((experts * half, width), BF16),
        ),
        (mixed, *packs, routes.T),
        2 * experts * half * width * tok_rows,
        16,
    )
    x = lax.all_to_all(
        sent.reshape(experts, half, width), "sp", split_axis=0, concat_axis=0, tiled=True
    ).reshape(held, width)

    acc_shape = (shape((held, 4 * units), F32), shape((held, 128), F32))
    chunk_flops = 2 * held * width * 4 * units
    acc, square = call(
        functools.partial(first_kernel, pack, chips), acc_shape, (x, gains, *packs), chunk_flops, 16
    )
    ahead, back = x, x
    last = chips // 2
    for step in range(1, last):
        ahead = along(ahead, 1)
        back = along(back, -1)
        acc, square = call(
            functools.partial(both_kernel, pack, chips, step),
            acc_shape,
            (ahead, back, gains, *packs, acc, square),
            2 * chunk_flops,
            16,
            {5: 0, 6: 1},
        )
    ahead = along(ahead, 1)
    _, _, hidden, ahead, back = call(
        functools.partial(last_kernel, pack, chips, float(total)),
        (*acc_shape, shape((held, CORES * units), BF16), *(shape((held, width), BF16),) * 2),
        (ahead, gains, *packs, acc, square),
        2 * chunk_flops,
        24,
        {4: 0, 5: 1},
    )

    def joined(part, came):
        return call(add_kernel, shape((held, width), BF16), (part, came), held * width, 8)

    steps = [*range(last - 1, -1, -1), *range(2 - last, 0)]
    parts = call(
        functools.partial(down_kernel, pack, chips, steps),
        (shape((held, width), F32),) * len(steps),
        (hidden, *packs),
        chunk_flops // 2 * len(steps),
        24,
    )
    part = dict(zip(steps, parts))
    for step in range(last - 1, -1, -1):
        ahead = along(ahead, -1, -1)
        if step:
            back = along(back, 1, -1)
            ahead = joined(part[step], ahead)
            back = joined(part[1 - step], back) if step > 1 else back
    result = call(own_kernel, pltpu.VMEM((held, width), BF16), (part[0], ahead, back), held * width, 8)
    returned = lax.all_to_all(
        result.reshape(blocks, half, width), "sp", split_axis=0, concat_axis=0, tiled=True
    ).reshape(experts * half, width)
    mine, theirs = call(
        functools.partial(pick_kernel, experts, capacity),
        (shape((tok_rows, features), F32),) * 2,
        (returned, routes.T, route_weight.T),
        4 * experts * half * width * tok_rows,
        12,
    )
    return call(
        join_kernel,
        shape((tok_rows, features), BF16),
        (stored, mine, across(theirs)),
        tok_rows * features,
        8,
    )


def solution(mesh):
    in_specs = (
        P("sp", "tp"),
        P("tp", None, None),
        P("tp"),
        P(None, "tp"),
        P("sp", "tp"),
        P("tp"),
        P("sp", None),
        P("sp", None),
        P("sp", None, "tp"),
        P("sp", None, "tp"),
        P("sp", "tp", None),
    )
    out_specs = P("sp", "tp")

    return jax.shard_map(on_device, mesh=mesh, in_specs=in_specs, out_specs=out_specs, check_vma=False)
```
